512 devices in a mesh: sp: 128 (over z, y, core), tp: 4 (over x).
Axes of the slice: x: 4, y: 8, z: 8, core: 2. Of those that a mesh axis runs over, the one named last changes fastest.
Arguments:
- tokens: bfloat16 [40960, 2048], P('sp', 'tp'), may hold values from -6 to 6
- pre_gain: float32 [2, 2048], replicated, may hold values from 0.1 to 1.9
- w_value: bfloat16 [2, 2048, 2048], P(None, 'sp', 'tp'), may hold values from -0.125 to 0.125
- w_gate: bfloat16 [2, 2048, 2048], P(None, 'sp', 'tp'), may hold values from -0.125 to 0.125
- taps: float32 [2, 31, 2048], P(None, None, 'tp'), may hold values from -5 to 5
- norm_gain: float32 [2, 2048], P(None, 'tp'), may hold values from 0.1 to 1.9
- norm_shift: float32 [2, 2048], P(None, 'tp'), may hold values from -3 to 3
- w_out: bfloat16 [2, 2048, 2048], P(None, 'tp', 'sp'), may hold values from -2 to 2
- post_gain: float32 [2, 2048], P(None, 'tp'), may hold values from 0.1 to 1.9
Outputs:
- stream: bfloat16 [40960, 2048], P('sp', 'tp')
The draws below stay inside these ranges and needn't reach their ends.
All inputs are finite; a program needn't handle non-finite values.
Results may differ from the reference program's by a relative error of at most 0.015.
Values may be sent and summed in bfloat16 or wider, within the bound.
A program may use at most 64 MiB of HBM per device.

```python
import jax
import jax.numpy as jnp
from jax import lax

D = 2048
CONV_WIDTH = 31
LAYERS = 2
TOKENS = 40960
N_TP = 4


def draw_taps(key, part):
    first, second, third = jax.random.split(jax.random.fold_in(key, 7), 3)
    base = jax.random.truncated_normal(first, -4.0, 4.0, (LAYERS, CONV_WIDTH, D), jnp.float32) * CONV_WIDTH ** (-0.5)
    channel = jnp.exp(jax.random.uniform(second, (LAYERS, 1, D), jnp.float32, -0.7, 0.7))
    levels = jnp.array([0.4, 0.8, 1.6, 3.2], jnp.float32)
    order = jnp.stack([jax.random.permutation(jax.random.fold_in(third, layer), 4) for layer in range(LAYERS)])
    groups = jnp.repeat(levels[order], D // 4, axis=1)
    return base * channel * groups[:, None, :]


def draw_w_out(key, part):
    first, second = jax.random.split(jax.random.fold_in(key, 11), 2)
    base = jax.random.truncated_normal(first, -4.0, 4.0, (LAYERS, D, D), jnp.float32) * D ** (-0.5)
    levels = jnp.array([0.4, 0.8, 1.6, 3.2], jnp.float32)
    order = jnp.stack([jax.random.permutation(jax.random.fold_in(second, layer), 4) for layer in range(LAYERS)])
    groups = jnp.repeat(levels[order], D // 4, axis=1)
    return (base * groups[:, None, :]).astype(jnp.bfloat16)


def shard_levels(own_key, shape, shards, low, largest):
    loudness = 1.0
    for position, parts in shards:
        draws = jax.random.uniform(jax.random.fold_in(jax.random.fold_in(own_key, 6), position), (parts,), jnp.float32, low / len(shards), largest / len(shards))
        loudness = loudness * jnp.repeat(jnp.exp(draws), shape[position] // parts).reshape((-1,) + (1,) * (len(shape) - 1 - position))
    return loudness


def noise(rng, shape, width, most, pieces=(), dtype=jnp.bfloat16):
    values = jax.random.normal(rng, shape, jnp.float32) * width
    if len(pieces) > 0:
        values = shard_levels(rng, shape, pieces, -0.22, 0.18) * values
    return jnp.clip(values, min=-most, max=most).astype(dtype)


def setup_inputs(seed: int = 0) -> dict:
    keys = jax.random.split(jax.random.key(seed), 10)
    tokens = noise(keys[0], (TOKENS, D), 1.0, 6.0, ((0, 128), (1, 4)))
    pre_gain = jnp.clip(1.0 + 0.18 * jax.random.normal(keys[1], (LAYERS, D), jnp.float32), 0.1, 1.9)
    w_value = noise(keys[2], (LAYERS, D, D), D ** -0.5, 0.125, ((1, 128), (2, 4)))
    w_gate = noise(keys[3], (LAYERS, D, D), D ** -0.5, 0.125, ((1, 128), (2, 4)))
    taps = draw_taps(jax.random.fold_in(keys[9], 71), 0)
    norm_gain = jnp.clip(1.0 + 0.18 * jax.random.normal(keys[5], (LAYERS, D), jnp.float32), 0.1, 1.9)
    norm_shift = noise(keys[6], (LAYERS, D), 0.5, 3.0, ((1, 4),), jnp.float32)
    w_out = draw_w_out(jax.random.fold_in(keys[9], 71), 0)
    post_gain = jnp.clip(1.0 + 0.18 * jax.random.normal(keys[8], (LAYERS, D), jnp.float32), 0.1, 1.9)
    return dict(tokens=tokens, pre_gain=pre_gain, w_value=w_value, w_gate=w_gate, taps=taps, norm_gain=norm_gain, norm_shift=norm_shift, w_out=w_out, post_gain=post_gain)


EPSILON = 1e-06
LN_EPSILON = 1e-05

def reference(tokens, pre_gain, w_value, w_gate, taps, norm_gain, norm_shift, w_out, post_gain):
    stream = tokens
    block = D // N_TP
    for layer in range(LAYERS):
        stream_f = stream.astype(jnp.float32)
        normed = (stream_f * lax.rsqrt(lax.optimization_barrier(jnp.mean(stream_f * stream_f, -1, keepdims=True)) + EPSILON) * pre_gain[layer]).astype(jnp.bfloat16)
        value_proj = jnp.dot(normed, w_value[layer], preferred_element_type=jnp.float32)
        gate_proj = jnp.dot(normed, w_gate[layer], preferred_element_type=jnp.float32)
        glu_act = (value_proj * jax.nn.sigmoid(gate_proj)).astype(jnp.bfloat16)
        padded = jnp.pad(glu_act.astype(jnp.float32), ((CONV_WIDTH - 1, 0), (0, 0)))
        conv_out = jnp.zeros((TOKENS, D), jnp.float32)
        for offset in range(CONV_WIDTH):
            conv_out = conv_out + taps[layer, offset] * padded[offset:offset + TOKENS]
        center = lax.optimization_barrier(jnp.sum(conv_out, -1, keepdims=True)) / D
        spread = jnp.maximum(lax.optimization_barrier(jnp.sum(conv_out * conv_out, -1, keepdims=True)) / D - center * center, 0.0)
        activated = jax.nn.silu((conv_out - center) * lax.rsqrt(spread + LN_EPSILON) * norm_gain[layer] + norm_shift[layer]).astype(jnp.bfloat16)
        summed = jnp.zeros((TOKENS, D), jnp.float32)
        for start in range(0, D, block):
            partial_sum = jnp.dot(activated[:, start:start + block], w_out[layer, start:start + block, :], preferred_element_type=jnp.float32).astype(jnp.bfloat16)
            partial_sum = lax.optimization_barrier(partial_sum)
            summed = summed + partial_sum.astype(jnp.float32)
        projected = summed.astype(jnp.bfloat16).astype(jnp.float32)
        scale = lax.rsqrt(lax.optimization_barrier(jnp.mean(projected * projected, -1, keepdims=True)) + EPSILON)
        stream = (stream_f + projected * scale * post_gain[layer]).astype(jnp.bfloat16)
    return stream
```

```python
import functools

import jax
import jax.numpy as jnp
from jax import lax
from jax.experimental import pallas as pl
from jax.experimental.pallas import tpu as pltpu
from jax.sharding import PartitionSpec as P

EPSILON = 1e-06
LN_EPSILON = 1e-05
HALO = 32
F32 = jnp.float32
BF16 = jnp.bfloat16
MESH = pl.DeviceIdType.MESH


class Geometry:
    def __init__(self, nz, ny, nc, nx, rows, ch, taps):
        self.nz, self.ny, self.nc, self.nx = nz, ny, nc, nx
        self.rows, self.ch, self.taps = rows, ch, taps
        self.d = ch * nx
        self.nsp = nz * ny * nc
        self.kr = self.d // self.nsp
        self.strips = ch // 128
        self.rp = -(-rows // 128) * 128
        self.rb = 64
        self.blocks = rows // self.rb


def body(
    g,
    tok, pre_gain, wv, wg, taps, ngain, nshift, wo, pgain,
    out,
    WV, WG, WO, X0, PJ, X1, NB, AV, AG, GF, FT, FR, CV, S1, S2, ACT, STB, SC, PG, T1, T2, R1, R2, OWN,
    wsend, wrecv, dsend, drecv, asend, arecv, rsend, rrecv, ssend, srecv, gsend, grecv, fsend, frecv,
):
    s = lax.axis_index("sp")
    x = lax.axis_index("tp")
    c = lax.rem(s, g.nc)
    y = lax.rem(lax.div(s, g.nc), g.ny)
    z = lax.div(s, g.nc * g.ny)
    sgn = 1 - 2 * c
    half = g.rows // 2
    top, bottom = pl.ds(0, half), pl.ds(half, half)

    def sp_of(zz, yy, cc):
        return (zz * g.ny + yy) * g.nc + cc

    def at_x(j):
        return lax.rem(x + j + g.nx, g.nx)

    def remote(src, dst, send, recv, sp=None, tp=None):
        return pltpu.make_async_remote_copy(
            src_ref=src, dst_ref=dst, send_sem=send, recv_sem=recv,
            device_id=(s if sp is None else sp, x if tp is None else tp),
            device_id_type=MESH,
        )

    sent = []

    def go(copy):
        copy.start()
        sent.append(copy)

    size = {"y": g.ny, "z": g.nz}
    here = {"y": y, "z": z}

    def moved(axis, by):
        n = size[axis]
        return lax.rem(here[axis] + by + 2 * n, n)

    def ring_sp(axis, by):
        p = moved(axis, by)
        return sp_of(z, p, c) if axis == "y" else sp_of(p, y, c)

    partner = sp_of(z, y, 1 - c)
    after = lax.rem(s + 1, g.nsp)
    before = lax.rem(s + g.nsp - 1, g.nsp)

    for layer in range(2):
        WV[z, y, c, layer] = wv[layer]
        WG[z, y, c, layer] = wg[layer]
        WO[z, y, c, layer] = wo[layer]
    PG[x] = jnp.broadcast_to(pgain[0:1, :], (8, g.ch))
    X0[x] = tok[...]
    STB[...] = jnp.zeros_like(STB)
    S1[...] = jnp.zeros_like(S1)
    S2[...] = jnp.zeros_like(S2)

    barrier = pltpu.get_barrier_semaphore()
    greet = [(None, at_x(j)) for j in range(1, g.nx)]
    greet += [(after, None), (before, None)]
    if g.nc > 1:
        greet.append((partner, None))
    for axis in ("y", "z"):
        if size[axis] > 1:
            greet += [(ring_sp(axis, 1), None), (ring_sp(axis, -1), None)]
    for sp, tp in greet:
        pl.semaphore_signal(
            barrier, inc=1,
            device_id=(s if sp is None else sp, x if tp is None else tp),
            device_id_type=MESH,
        )
    pl.semaphore_wait(barrier, len(greet))

    order = (("y", "z"), ("z", "y"))
    lanes = g.ch // 2

    def source(item, stream):
        if item % 2 == 0:
            return (WV, WG)[stream], pl.ds(0, g.ch)
        return WO, pl.ds(stream * lanes, lanes)

    def block(item, stream, phase, pos, core):
        buf, cols = source(item, stream)
        layer = item // 2
        if phase == 0:
            zz, yy = (z, pos) if stream == 0 else (pos, y)
            return buf.at[zz, yy, core, layer, :, cols]
        if stream == 0:
            return buf.at[pos, :, core, layer, :, cols]
        return buf.at[:, pos, core, layer, :, cols]

    def hops(axis):
        n = size[axis]
        return (n // 2, n - 1 - n // 2)

    def ring_copy(item, stream, phase, way, step):
        axis = order[stream][phase]
        toward = sgn if way == 0 else -sgn
        ref = block(item, stream, phase, moved(axis, -toward * step), c)
        return remote(
            ref, ref,
            wsend.at[item, stream, phase, way, step],
            wrecv.at[item, stream, phase, way, step],
            sp=ring_sp(axis, toward),
        )

    def arrival(item, stream, phase, way, step):
        axis = order[stream][phase]
        toward = sgn if way == 0 else -sgn
        ref = block(item, stream, phase, moved(axis, -toward * (step + 1)), c)
        remote(
            ref, ref,
            wsend.at[item, stream, phase, way, step],
            wrecv.at[item, stream, phase, way, step],
            sp=ring_sp(axis, toward),
        ).wait_recv()

    def across(item, stream, index, pos):
        if g.nc > 1:
            ref = block(item, stream, 1, pos, c)
            go(remote(ref, ref, dsend.at[item, stream, index], drecv.at[item, stream, index], sp=partner))

    def begin(item, phase):
        for stream in range(2):
            axis = order[stream][phase]
            for way in range(2):
                if hops(axis)[way] > 0:
                    go(ring_copy(item, stream, phase, way, 0))
            if phase == 1:
                across(item, stream, 0, here[axis])

    def advance(item, phase, step):
        for stream in range(2):
            axis = order[stream][phase]
            for way in range(2):
                if step < hops(axis)[way]:
                    arrival(item, stream, phase, way, step)
                    if step + 1 < hops(axis)[way]:
                        go(ring_copy(item, stream, phase, way, step + 1))
                    if phase == 1:
                        toward = sgn if way == 0 else -sgn
                        across(
                            item, stream, 1 + way * hops(axis)[0] + step,
                            moved(axis, -toward * (step + 1)),
                        )

    def finish(item):
        if g.nc > 1:
            for stream in range(2):
                axis = order[stream][1]
                for index in range(size[axis]):
                    ref = block(item, stream, 1, index, 1 - c)
                    remote(
                        ref, ref, dsend.at[item, stream, index], drecv.at[item, stream, index], sp=partner
                    ).wait_recv()

    steps = max(g.ny, g.nz) // 2

    ways = ((1, top, bottom), (-1, bottom, top))

    def spread_copy(layer, buf, way, piece):
        toward, first, second = ways[way]
        slot, part = ((x, first), (x, second), (at_x(-toward), first))[piece]
        ref = buf.at[slot, part]
        return remote(
            ref, ref, asend.at[layer, way, piece], arecv.at[layer, way, piece], tp=at_x(toward)
        )

    def spread_begin(layer, buf):
        for piece in range(2):
            for way in range(2):
                go(spread_copy(layer, buf, way, piece))

    def spread_wait(layer, buf, way, piece):
        toward, first, second = ways[way]
        slot, part = ((at_x(-toward), first), (at_x(-toward), second), (at_x(-2 * toward), first))[piece]
        ref = buf.at[slot, part]
        remote(
            ref, ref, asend.at[layer, way, piece], arecv.at[layer, way, piece], tp=at_x(toward)
        ).wait_recv()

    def spread_relay(layer, buf):
        for way in range(2):
            spread_wait(layer, buf, way, 0)
            go(spread_copy(layer, buf, way, 2))

    def spread_end(layer, buf):
        for piece in (1, 2):
            for way in range(2):
                spread_wait(layer, buf, way, piece)

    def tell(which):
        for j in range(1, g.nx):
            ref = STB.at[which, x]
            go(remote(ref, ref, ssend.at[which, j - 1], srecv.at[which, j - 1], tp=at_x(j)))

    def told(which):
        for j in range(1, g.nx):
            ref = STB.at[which, at_x(-j)]
            remote(ref, ref, ssend.at[which, j - 1], srecv.at[which, j - 1], tp=at_x(j)).wait_recv()

    def row_sums(buf):
        return jnp.sum(jnp.transpose(buf[...]), axis=0, keepdims=True)

    def as_columns(which, row):
        SC[which] = jnp.transpose(jnp.broadcast_to(row, (128, g.rp)))

    for item in (0, 1):
        begin(item, 0)
    spread_begin(0, X0)
    for item in (2, 3):
        begin(item, 0)
    for j in range(1, g.nx):
        go(remote(PG.at[x], PG.at[x], gsend.at[j - 1], grecv.at[j - 1], tp=at_x(j)))
    for step in range(steps):
        for item in (0, 1):
            advance(item, 0, step)
    begin(0, 1)
    begin(1, 1)
    spread_relay(0, X0)
    for step in range(steps):
        for item in (2, 3):
            advance(item, 0, step)
    advance(0, 1, 0)
    advance(1, 1, 0)
    spread_end(0, X0)

    def norm_rows(layer):
        def at(i, carry):
            rows = pl.ds(i * g.rb, g.rb)
            if layer == 1:
                square = jnp.zeros((g.rb, 1), F32)
                for j in range(g.nx):
                    v = PJ[j, rows, :].astype(F32)
                    square += jnp.sum(v * v, -1, keepdims=True)
                scale = lax.rsqrt(square / g.d + EPSILON)
            total = jnp.zeros((g.rb, 1), F32)
            for j in range(g.nx):
                v = X0[j, rows, :].astype(F32)
                if layer == 1:
                    v = v + PJ[j, rows, :].astype(F32) * scale * PG[j, 0:1, :]
                    X1[j, rows, :] = v.astype(BF16)
                    v = v.astype(BF16).astype(F32)
                total += jnp.sum(v * v, -1, keepdims=True)
            inv = lax.rsqrt(total / g.d + EPSILON)
            for j in range(g.nx):
                v = (X0, X1)[layer][j, rows, :].astype(F32)
                cols = pl.ds(j * g.ch, g.ch)
                NB[j, rows, :] = (v * inv * pre_gain[layer : layer + 1, cols]).astype(BF16)
            return carry

        lax.fori_loop(0, g.blocks, at, 0)

    zs = g.nz // g.nx

    def project_in(layer):
        for n, (acc, w) in enumerate(((AV, WV), (AG, WG))):
            def at(j, carry):
                mat = w[pl.ds(j * zs, zs), :, :, layer].reshape(g.ch, g.ch)
                acc[...] += jnp.dot(NB[j], mat, preferred_element_type=F32)
                return carry

            mat = w[0:zs, :, :, layer].reshape(g.ch, g.ch)
            acc[...] = jnp.dot(NB[0], mat, preferred_element_type=F32)
            lax.fori_loop(1, g.nx, at, 0)

    def gate(i, carry):
        rows = pl.ds(i * g.rb, g.rb)
        for k in range(g.strips):
            cols = pl.ds(k * 128, 128)
            act = (AV[rows, cols] * jax.nn.sigmoid(AG[rows, cols])).astype(BF16)
            GF[k, pl.ds(HALO + i * g.rb, g.rb), :] = act.astype(F32)
        return carry

    def fringe_copy(layer):
        return remote(FT.at[layer], FR.at[layer], fsend.at[layer], frecv.at[layer], sp=after)

    def convolve(layer, i):
        whole = [jnp.zeros((g.rb, 128), F32) for _ in range(2)]
        for k in range(g.strips):
            cols = pl.ds(k * 128, 128)
            acc = jnp.zeros((g.rb, 128), F32)
            for tap in range(g.taps):
                rows = pl.ds(i * g.rb + (HALO - g.taps + 1 + tap), g.rb)
                acc = acc + taps[layer, tap : tap + 1, cols] * GF[k, rows, :]
            CV[k, pl.ds(i * g.rb, g.rb), :] = acc
            whole = [whole[0] + acc, whole[1] + acc * acc]
        S1[pl.ds(i * g.rb, g.rb), :] = whole[0]
        S2[pl.ds(i * g.rb, g.rb), :] = whole[1]

    def activate(layer, i):
        rows = pl.ds(i * g.rb, g.rb)
        center = SC[0, rows, :]
        inv = SC[1, rows, :]
        for k in range(g.strips):
            cols = pl.ds(k * 128, 128)
            v = (CV[k, rows, :] - center) * inv * ngain[layer : layer + 1, cols] + nshift[
                layer : layer + 1, cols
            ]
            ACT[rows, cols] = (v * jax.nn.sigmoid(v)).astype(BF16)

    def part_for(layer, dest):
        mat = WO[pl.ds(dest * zs, zs), :, :, layer].reshape(g.ch, g.ch)
        return lax.dot_general(ACT[...], mat, (((1,), (1,)), ((), ())), preferred_element_type=F32)

    def loop(fn, lo, hi):
        def at(i, carry):
            fn(i)
            return carry

        lax.fori_loop(lo, hi, at, 0)

    pending = []
    for step in range(1, steps):
        pending.append([lambda st=step, it=it: advance(it, 1, st) for it in (0, 1)])
    pump_first = pending
    later = [lambda: (begin(2, 1), begin(3, 1))]
    for step in range(steps):
        later += [lambda st=step: advance(2, 1, st), lambda st=step: advance(3, 1, st)]

    def pump(n):
        for _ in range(n):
            if later:
                later.pop(0)()

    for layer in range(2):
        if layer == 1:
            spread_relay(1, PJ)
            spread_end(1, PJ)
        norm_rows(layer)
        if layer == 0:
            for group in pump_first:
                for event in group:
                    event()
            pump(1)
            finish(0)
            finish(1)
        else:
            pump(len(later))
            finish(2)
            finish(3)
        project_in(layer)
        lax.fori_loop(0, g.blocks, gate, 0)
        for k in range(g.strips):
            FT[layer, :, k * 128 : (k + 1) * 128] = GF[k, g.rows : g.rows + HALO, :].astype(BF16)
        if layer == 0:
            pump(2)
        go(fringe_copy(layer))
        loop(lambda i: convolve(layer, i), 1, g.blocks)
        fringe_copy(layer).wait_recv()
        keep = jnp.where(s > 0, 1.0, 0.0).astype(F32)
        for k in range(g.strips):
            GF[k, 0:HALO, :] = FR[layer, :, k * 128 : (k + 1) * 128].astype(F32) * keep
        loop(lambda i: convolve(layer, i), 0, 1)
        STB[layer, x, 0:1, :] = row_sums(S1)
        STB[layer, x, 1:2, :] = row_sums(S2)
        tell(layer)
        if layer == 0:
            pump(2)
        told(layer)
        sums = STB[layer, 0]
        for j in range(1, g.nx):
            sums = sums + STB[layer, j]
        center = sums[0:1, :] / g.d
        spread = jnp.maximum(sums[1:2, :] / g.d - center * center, 0.0)
        as_columns(0, center)
        as_columns(1, lax.rsqrt(spread + LN_EPSILON))
        loop(lambda i: activate(layer, i), 0, g.blocks)

        def rs(index, src, dst, toward):
            return remote(src, dst, rsend.at[layer, index], rrecv.at[layer, index], tp=at_x(toward))

        hop = (
            rs(0, T1.at[layer, top], R1.at[layer, 0], 1),
            rs(1, T1.at[layer, bottom], R1.at[layer, 1], -1),
            rs(2, T2.at[layer, 0], R2.at[layer, 0], 1),
            rs(3, T2.at[layer, 1], R2.at[layer, 1], -1),
        )
        T1[layer] = part_for(layer, at_x(2)).astype(BF16)
        go(hop[0])
        go(hop[1])
        OWN[...] = part_for(layer, at_x(1))
        hop[0].wait_recv()
        T2[layer, 0, top] = (OWN[top] + R1[layer, 0].astype(F32)).astype(BF16)
        T2[layer, 0, bottom] = OWN[bottom].astype(BF16)
        go(hop[2])
        OWN[...] = part_for(layer, at_x(-1))
        hop[1].wait_recv()
        T2[layer, 1, bottom] = (OWN[bottom] + R1[layer, 1].astype(F32)).astype(BF16)
        T2[layer, 1, top] = OWN[top].astype(BF16)
        go(hop[3])
        OWN[...] = part_for(layer, x)
        if layer == 0:
            pump(2)
        hop[2].wait_recv()
        hop[3].wait_recv()

        def combine(i):
            rows = pl.ds(i * g.rb, g.rb)
            v = (OWN[rows] + R2[layer, 0, rows].astype(F32) + R2[layer, 1, rows].astype(F32)).astype(BF16)
            if layer == 0:
                PJ[x, rows, :] = v
            else:
                T1[0, rows, :] = v
                v = v.astype(F32)
                v = v * v
                S1[rows, :] = sum(v[:, k * 128 : (k + 1) * 128] for k in range(g.strips))

        if layer == 0:
            loop(combine, 0, g.blocks)
            for j in range(1, g.nx):
                ref = PG.at[at_x(-j)]
                remote(ref, ref, gsend.at[j - 1], grecv.at[j - 1], tp=at_x(j)).wait_recv()
            spread_begin(1, PJ)
        else:
            rs_done = [hop_ for hop_ in sent]
            for copy in rs_done:
                copy.wait_send()
            sent.clear()
            loop(combine, 0, g.blocks)

    STB[2, x, 0:1, :] = row_sums(S1)
    tell(2)
    told(2)
    square = sum(STB[2, j, 0:1, :] for j in range(g.nx))
    as_columns(0, lax.rsqrt(square / g.d + EPSILON))

    def last(i):
        rows = pl.ds(i * g.rb, g.rb)
        for k in range(g.strips):
            cols = pl.ds(k * 128, 128)
            v = T1[0, rows, cols].astype(F32) * SC[0, rows, :] * pgain[1:2, cols]
            out[rows, cols] = (X1[x, rows, cols].astype(F32) + v).astype(BF16)

    loop(last, 0, g.blocks)
    for copy in sent:
        copy.wait_send()


def local(g, tokens, pre_gain, w_value, w_gate, taps, norm_gain, norm_shift, w_out, post_gain):
    w_out = jnp.swapaxes(w_out, 1, 2)
    vm = pl.BlockSpec(memory_space=pltpu.VMEM)
    slots = (g.nz, g.ny, g.nc, 2, g.kr, g.ch)
    rows, ch = g.rows, g.ch
    most = max(g.ny, g.nz)
    dma = pltpu.SemaphoreType.DMA
    scratch = [
        pltpu.VMEM(slots, BF16),
        pltpu.VMEM(slots, BF16),
        pltpu.VMEM(slots, BF16),
        pltpu.VMEM((g.nx, rows, ch), BF16),
        pltpu.VMEM((g.nx, rows, ch), BF16),
        pltpu.VMEM((g.nx, rows, ch), BF16),
        pltpu.VMEM((g.nx, rows, ch), BF16),
        pltpu.VMEM((rows, ch), F32),
        pltpu.VMEM((rows, ch), F32),
        pltpu.VMEM((g.strips, HALO + rows, 128), F32),
        pltpu.VMEM((2, HALO, ch), BF16),
        pltpu.VMEM((2, HALO, ch), BF16),
        pltpu.VMEM((g.strips, rows, 128), F32),
        pltpu.VMEM((g.rp, 128), F32),
        pltpu.VMEM((g.rp, 128), F32),
        pltpu.VMEM((rows, ch), BF16),
        pltpu.VMEM((3, g.nx, 8, g.rp), F32),
        pltpu.VMEM((2, g.rp, 128), F32),
        pltpu.VMEM((g.nx, 8, ch), F32),
        pltpu.VMEM((2, rows, ch), BF16),
        pltpu.VMEM((2, 2, rows, ch), BF16),
        pltpu.VMEM((2, 2, rows // 2, ch), BF16),
        pltpu.VMEM((2, 2, rows, ch), BF16),
        pltpu.VMEM((rows, ch), F32),
        dma((4, 2, 2, 2, most // 2)),
        dma((4, 2, 2, 2, most // 2)),
        dma((4, 2, most)),
        dma((4, 2, most)),
        dma((2, 2, 3)),
        dma((2, 2, 3)),
        dma((2, 4)),
        dma((2, 4)),
        dma((3, 3)),
        dma((3, 3)),
        dma((3,)),
        dma((3,)),
        dma((2,)),
        dma((2,)),
    ]
    return pl.pallas_call(
        functools.partial(body, g),
        out_shape=jax.ShapeDtypeStruct((rows, ch), BF16),
        in_specs=[vm] * 9,
        out_specs=vm,
        scratch_shapes=scratch,
        compiler_params=pltpu.CompilerParams(
            collective_id=0, has_side_effects=True, vmem_limit_bytes=60 * 1024 * 1024
        ),
    )(tokens, pre_gain, w_value, w_gate, taps, norm_gain, norm_shift, w_out, post_gain)


def build(mesh, sizes, rows, ch, width):
    g = Geometry(*sizes, mesh.shape["tp"], rows, ch, width)
    placed = (
        P("sp", "tp"),
        P(),
        P(None, "sp", "tp"),
        P(None, "sp", "tp"),
        P(None, None, "tp"),
        P(None, "tp"),
        P(None, "tp"),
        P(None, "tp", "sp"),
        P(None, "tp"),
    )
    return jax.shard_map(
        functools.partial(local, g), mesh=mesh, in_specs=placed, out_specs=P("sp", "tp"), check_vma=False
    )


def solution(mesh):
    return build(mesh, (8, 8, 2), 320, 512, 31)
```

```python
import functools

import jax
import jax.numpy as jnp
from jax import lax
from jax.experimental import pallas as pl
from jax.experimental.pallas import tpu as pltpu
from jax.sharding import PartitionSpec as P

EPSILON = 1e-06
LN_EPSILON = 1e-05
HALO = 32
F32 = jnp.float32
BF16 = jnp.bfloat16
MESH = pl.DeviceIdType.MESH


class Geometry:
    def __init__(self, nz, ny, nc, nx, rows, ch, taps):
        self.nz, self.ny, self.nc, self.nx = nz, ny, nc, nx
        self.rows, self.ch, self.taps = rows, ch, taps
        self.d = ch * nx
        self.nsp = nz * ny * nc
        self.kr = self.d // self.nsp
        self.strips = ch // 128
        self.rp = -(-rows // 128) * 128
        self.rb = 64
        self.blocks = rows // self.rb


def body(
    g,
    tok, pre_gain, wv, wg, taps, ngain, nshift, wo, pgain,
    out,
    WV, WG, WO, X0, PJ, X1, NB, AV, AG, GF, FT, FR, CV, S1, S2, ACT, STB, SC, PG, T1, T2, R1, R2, OWN,
    esend, erecv, wsend, wrecv, dsend, drecv, asend, arecv, rsend, rrecv, ssend, srecv, gsend, grecv, fsend, frecv,
):
    s = lax.axis_index("sp")
    x = lax.axis_index("tp")
    c = lax.rem(s, g.nc)
    y = lax.rem(lax.div(s, g.nc), g.ny)
    z = lax.div(s, g.nc * g.ny)
    sgn = 1 - 2 * c
    half = g.rows // 2
    top, bottom = pl.ds(0, half), pl.ds(half, half)

    def sp_of(zz, yy, cc):
        return (zz * g.ny + yy) * g.nc + cc

    def at_x(j):
        return lax.rem(x + j + g.nx, g.nx)

    def remote(src, dst, send, recv, sp=None, tp=None):
        return pltpu.make_async_remote_copy(
            src_ref=src, dst_ref=dst, send_sem=send, recv_sem=recv,
            device_id=(s if sp is None else sp, x if tp is None else tp),
            device_id_type=MESH,
        )

    sent = []

    def go(copy):
        copy.start()
        sent.append(copy)

    size = {"y": g.ny, "z": g.nz}
    here = {"y": y, "z": z}

    def moved(axis, by):
        n = size[axis]
        return lax.rem(here[axis] + by + 2 * n, n)

    def ring_sp(axis, by):
        p = moved(axis, by)
        return sp_of(z, p, c) if axis == "y" else sp_of(p, y, c)

    partner = sp_of(z, y, 1 - c)
    after = lax.rem(s + 1, g.nsp)
    before = lax.rem(s + g.nsp - 1, g.nsp)

    for layer in range(2):
        WV[z, y, c, layer] = wv[layer]
        WG[z, y, c, layer] = wg[layer]
        WO[z, y, c, layer] = wo[layer]
    PG[x] = jnp.broadcast_to(pgain[0:1, :], (8, g.ch))
    X0[x] = tok[...]
    STB[...] = jnp.zeros_like(STB)
    S1[...] = jnp.zeros_like(S1)
    S2[...] = jnp.zeros_like(S2)

    barrier = pltpu.get_barrier_semaphore()
    greet = [(None, at_x(j)) for j in range(1, g.nx)]
    greet += [(after, None), (before, None)]
    if g.nc > 1:
        greet.append((partner, None))
    for axis in ("y", "z"):
        greet += [(ring_sp(axis, k), None) for k in range(1, size[axis])]
    for sp, tp in greet:
        pl.semaphore_signal(
            barrier, inc=1,
            device_id=(s if sp is None else sp, x if tp is None else tp),
            device_id_type=MESH,
        )
    pl.semaphore_wait(barrier, len(greet))

    order = (("y", "z"), ("z", "y"))
    lanes = g.ch // 2
    pieces = {0: (0, 1), 1: (2,), 2: (3, 4), 3: (5,)}

    def source(item, stream):
        if item % 2 == 0:
            return (WV, WG)[stream], pl.ds(0, g.ch)
        return WO, pl.ds(stream * lanes, lanes)

    def own_slot(item, stream, pos):
        buf, cols = source(item, stream)
        zz, yy = (z, pos) if stream == 0 else (pos, y)
        return buf.at[zz, yy, c, item // 2, :, cols]

    def block(item, stream, pos, core, piece=None):
        buf, cols = source(item, stream)
        across_dim = slice(None)
        if piece is not None and len(pieces[item]) == 2:
            n = size[order[stream][0]] // 2
            near = lax.div(here[order[stream][0]], n)
            across_dim = pl.ds((near if piece == pieces[item][0] else 1 - near) * n, n)
        if stream == 0:
            return buf.at[pos, across_dim, core, item // 2, :, cols]
        return buf.at[across_dim, pos, core, item // 2, :, cols]

    def hops(axis):
        n = size[axis]
        return (n // 2, n - 1 - n // 2)

    def scatter_copy(item, stream, k):
        axis = order[stream][0]
        ref = own_slot(item, stream, here[axis])
        return remote(ref, ref, esend.at[item, stream, k], erecv.at[item, stream, k], sp=ring_sp(axis, k))

    def farthest_first(n):
        return sorted(range(1, n), key=lambda k: -min(k, n - k))

    def scatter(item):
        for k in farthest_first(max(g.ny, g.nz)):
            for stream in range(2):
                if k < size[order[stream][0]]:
                    go(scatter_copy(item, stream, k))

    def scattered(item):
        for stream in range(2):
            axis = order[stream][0]
            for k in range(1, size[axis]):
                ref = own_slot(item, stream, moved(axis, -k))
                remote(
                    ref, ref, esend.at[item, stream, k], erecv.at[item, stream, k], sp=ring_sp(axis, k)
                ).wait_recv()

    def ring_copy(item, piece, stream, way, step, back):
        axis = order[stream][1]
        toward = sgn if way == 0 else -sgn
        ref = block(item, stream, moved(axis, -toward * (step + back)), c, piece)
        return remote(
            ref, ref,
            wsend.at[piece, stream, way, step],
            wrecv.at[piece, stream, way, step],
            sp=ring_sp(axis, toward),
        )

    def across(item, stream, index, pos):
        if g.nc > 1:
            ref = block(item, stream, pos, c)
            go(remote(ref, ref, dsend.at[item, stream, index], drecv.at[item, stream, index], sp=partner))

    def begin(item):
        for piece in pieces[item]:
            for stream in range(2):
                axis = order[stream][1]
                for way in range(2):
                    if hops(axis)[way] > 0:
                        go(ring_copy(item, piece, stream, way, 0, 0))
        for stream in range(2):
            across(item, stream, 0, here[order[stream][1]])

    def advance(item, step):
        for piece in pieces[item]:
            for stream in range(2):
                axis = order[stream][1]
                for way in range(2):
                    if step < hops(axis)[way]:
                        ring_copy(item, piece, stream, way, step, 1).wait_recv()
                        if step + 1 < hops(axis)[way]:
                            go(ring_copy(item, piece, stream, way, step + 1, 0))
                        if piece == pieces[item][-1]:
                            toward = sgn if way == 0 else -sgn
                            across(
                                item, stream, 1 + way * hops(axis)[0] + step,
                                moved(axis, -toward * (step + 1)),
                            )

    def finish(item):
        if g.nc > 1:
            for stream in range(2):
                axis = order[stream][1]
                for index in range(size[axis]):
                    ref = block(item, stream, index, 1 - c)
                    remote(
                        ref, ref, dsend.at[item, stream, index], drecv.at[item, stream, index], sp=partner
                    ).wait_recv()

    steps = max(g.ny, g.nz) // 2

    ways = ((1, top, bottom), (-1, bottom, top))

    def spread_copy(layer, buf, way, piece):
        toward, first, second = ways[way]
        slot, part = ((x, first), (x, second), (at_x(-toward), first))[piece]
        ref = buf.at[slot, part]
        return remote(
            ref, ref, asend.at[layer, way, piece], arecv.at[layer, way, piece], tp=at_x(toward)
        )

    def spread_begin(layer, buf):
        for piece in range(2):
            for way in range(2):
                go(spread_copy(layer, buf, way, piece))

    def spread_wait(layer, buf, way, piece):
        toward, first, second = ways[way]
        slot, part = ((at_x(-toward), first), (at_x(-toward), second), (at_x(-2 * toward), first))[piece]
        ref = buf.at[slot, part]
        remote(
            ref, ref, asend.at[layer, way, piece], arecv.at[layer, way, piece], tp=at_x(toward)
        ).wait_recv()

    def spread_relay(layer, buf):
        for way in range(2):
            spread_wait(layer, buf, way, 0)
            go(spread_copy(layer, buf, way, 2))

    def spread_end(layer, buf):
        for piece in (1, 2):
            for way in range(2):
                spread_wait(layer, buf, way, piece)

    def tell(which):
        for j in range(1, g.nx):
            ref = STB.at[which, x]
            go(remote(ref, ref, ssend.at[which, j - 1], srecv.at[which, j - 1], tp=at_x(j)))

    def told(which):
        for j in range(1, g.nx):
            ref = STB.at[which, at_x(-j)]
            remote(ref, ref, ssend.at[which, j - 1], srecv.at[which, j - 1], tp=at_x(j)).wait_recv()

    def row_sums(buf):
        return jnp.sum(jnp.transpose(buf[...]), axis=0, keepdims=True)

    def as_columns(which, row):
        SC[which] = jnp.transpose(jnp.broadcast_to(row, (128, g.rp)))

    scatter(0)
    spread_begin(0, X0)
    scatter(1)
    for j in range(1, g.nx):
        go(remote(PG.at[x], PG.at[x], gsend.at[j - 1], grecv.at[j - 1], tp=at_x(j)))
    scattered(0)
    begin(0)
    scattered(1)
    begin(1)
    scatter(2)
    scatter(3)
    spread_relay(0, X0)
    advance(0, 0)
    advance(1, 0)
    spread_end(0, X0)

    def norm_rows(layer):
        def at(i, carry):
            rows = pl.ds(i * g.rb, g.rb)
            if layer == 1:
                square = jnp.zeros((g.rb, 1), F32)
                for j in range(g.nx):
                    v = PJ[j, rows, :].astype(F32)
                    square += jnp.sum(v * v, -1, keepdims=True)
                scale = lax.rsqrt(square / g.d + EPSILON)
            total = jnp.zeros((g.rb, 1), F32)
            for j in range(g.nx):
                v = X0[j, rows, :].astype(F32)
                if layer == 1:
                    v = v + PJ[j, rows, :].astype(F32) * scale * PG[j, 0:1, :]
                    X1[j, rows, :] = v.astype(BF16)
                    v = v.astype(BF16).astype(F32)
                total += jnp.sum(v * v, -1, keepdims=True)
            inv = lax.rsqrt(total / g.d + EPSILON)
            for j in range(g.nx):
                v = (X0, X1)[layer][j, rows, :].astype(F32)
                cols = pl.ds(j * g.ch, g.ch)
                NB[j, rows, :] = (v * inv * pre_gain[layer : layer + 1, cols]).astype(BF16)
            return carry

        lax.fori_loop(0, g.blocks, at, 0)

    zs = g.nz // g.nx

    def project_in(layer):
        for n, (acc, w) in enumerate(((AV, WV), (AG, WG))):
            def at(j, carry):
                mat = w[pl.ds(j * zs, zs), :, :, layer].reshape(g.ch, g.ch)
                acc[...] += jnp.dot(NB[j], mat, preferred_element_type=F32)
                return carry

            mat = w[0:zs, :, :, layer].reshape(g.ch, g.ch)
            acc[...] = jnp.dot(NB[0], mat, preferred_element_type=F32)
            lax.fori_loop(1, g.nx, at, 0)

    def gate(i, carry):
        rows = pl.ds(i * g.rb, g.rb)
        for k in range(g.strips):
            cols = pl.ds(k * 128, 128)
            act = (AV[rows, cols] * jax.nn.sigmoid(AG[rows, cols])).astype(BF16)
            GF[k, pl.ds(HALO + i * g.rb, g.rb), :] = act.astype(F32)
        return carry

    def fringe_copy(layer):
        return remote(FT.at[layer], FR.at[layer], fsend.at[layer], frecv.at[layer], sp=after)

    def convolve(layer, i):
        whole = [jnp.zeros((g.rb, 128), F32) for _ in range(2)]
        for k in range(g.strips):
            cols = pl.ds(k * 128, 128)
            acc = jnp.zeros((g.rb, 128), F32)
            for tap in range(g.taps):
                rows = pl.ds(i * g.rb + (HALO - g.taps + 1 + tap), g.rb)
                acc = acc + taps[tap, layer : layer + 1, cols] * GF[k, rows, :]
            CV[k, pl.ds(i * g.rb, g.rb), :] = acc
            whole = [whole[0] + acc, whole[1] + acc * acc]
        S1[pl.ds(i * g.rb, g.rb), :] = whole[0]
        S2[pl.ds(i * g.rb, g.rb), :] = whole[1]

    def activate(layer, i):
        rows = pl.ds(i * g.rb, g.rb)
        center = SC[0, rows, :]
        inv = SC[1, rows, :]
        for k in range(g.strips):
            cols = pl.ds(k * 128, 128)
            v = (CV[k, rows, :] - center) * inv * ngain[layer : layer + 1, cols] + nshift[
                layer : layer + 1, cols
            ]
            ACT[rows, cols] = (v * jax.nn.sigmoid(v)).astype(BF16)

    def part_for(layer, dest):
        mat = WO[pl.ds(dest * zs, zs), :, :, layer].reshape(g.ch, g.ch)
        return lax.dot_general(ACT[...], mat, (((1,), (1,)), ((), ())), preferred_element_type=F32)

    def loop(fn, lo, hi):
        def at(i, carry):
            fn(i)
            return carry

        lax.fori_loop(lo, hi, at, 0)

    later = [lambda: (scattered(2), begin(2), scattered(3), begin(3))]
    for step in range(steps):
        later += [lambda st=step: advance(2, st), lambda st=step: advance(3, st)]

    def pump(n):
        for _ in range(n):
            if later:
                later.pop(0)()

    for layer in range(2):
        if layer == 1:
            spread_relay(1, PJ)
            spread_end(1, PJ)
        norm_rows(layer)
        if layer == 0:
            for step in range(1, steps):
                advance(0, step)
                advance(1, step)
            pump(1)
            finish(0)
            finish(1)
        else:
            pump(len(later))
            finish(2)
            finish(3)
        project_in(layer)
        lax.fori_loop(0, g.blocks, gate, 0)
        for k in range(g.strips):
            FT[layer, :, k * 128 : (k + 1) * 128] = GF[k, g.rows : g.rows + HALO, :].astype(BF16)
        if layer == 0:
            pump(2)
        go(fringe_copy(layer))
        loop(lambda i: convolve(layer, i), 1, g.blocks)
        fringe_copy(layer).wait_recv()
        keep = jnp.where(s > 0, 1.0, 0.0).astype(F32)
        for k in range(g.strips):
            GF[k, 0:HALO, :] = FR[layer, :, k * 128 : (k + 1) * 128].astype(F32) * keep
        loop(lambda i: convolve(layer, i), 0, 1)
        STB[layer, x, 0:1, :] = row_sums(S1)
        STB[layer, x, 1:2, :] = row_sums(S2)
        tell(layer)
        if layer == 0:
            pump(2)
        told(layer)
        sums = STB[layer, 0]
        for j in range(1, g.nx):
            sums = sums + STB[layer, j]
        center = sums[0:1, :] / g.d
        spread = jnp.maximum(sums[1:2, :] / g.d - center * center, 0.0)
        as_columns(0, center)
        as_columns(1, lax.rsqrt(spread + LN_EPSILON))
        loop(lambda i: activate(layer, i), 0, g.blocks)

        def rs(index, src, dst, toward):
            return remote(src, dst, rsend.at[layer, index], rrecv.at[layer, index], tp=at_x(toward))

        hop = (
            rs(0, T1.at[layer, top], R1.at[layer, 0], 1),
            rs(1, T1.at[layer, bottom], R1.at[layer, 1], -1),
            rs(2, T2.at[layer, 0], R2.at[layer, 0], 1),
            rs(3, T2.at[layer, 1], R2.at[layer, 1], -1),
        )
        T1[layer] = part_for(layer, at_x(2)).astype(BF16)
        go(hop[0])
        go(hop[1])
        OWN[...] = part_for(layer, at_x(1))
        hop[0].wait_recv()
        T2[layer, 0, top] = (OWN[top] + R1[layer, 0].astype(F32)).astype(BF16)
        T2[layer, 0, bottom] = OWN[bottom].astype(BF16)
        go(hop[2])
        OWN[...] = part_for(layer, at_x(-1))
        hop[1].wait_recv()
        T2[layer, 1, bottom] = (OWN[bottom] + R1[layer, 1].astype(F32)).astype(BF16)
        T2[layer, 1, top] = OWN[top].astype(BF16)
        go(hop[3])
        OWN[...] = part_for(layer, x)
        if layer == 0:
            pump(2)
        hop[2].wait_recv()
        hop[3].wait_recv()

        def combine(i):
            rows = pl.ds(i * g.rb, g.rb)
            v = (OWN[rows] + R2[layer, 0, rows].astype(F32) + R2[layer, 1, rows].astype(F32)).astype(BF16)
            if layer == 0:
                PJ[x, rows, :] = v
            else:
                T1[0, rows, :] = v
                v = v.astype(F32)
                v = v * v
                S1[rows, :] = sum(v[:, k * 128 : (k + 1) * 128] for k in range(g.strips))

        if layer == 0:
            loop(combine, 0, g.blocks)
            for j in range(1, g.nx):
                ref = PG.at[at_x(-j)]
                remote(ref, ref, gsend.at[j - 1], grecv.at[j - 1], tp=at_x(j)).wait_recv()
            spread_begin(1, PJ)
        else:
            rs_done = [hop_ for hop_ in sent]
            for copy in rs_done:
                copy.wait_send()
            sent.clear()
            loop(combine, 0, g.blocks)

    STB[2, x, 0:1, :] = row_sums(S1)
    tell(2)
    told(2)
    square = sum(STB[2, j, 0:1, :] for j in range(g.nx))
    as_columns(0, lax.rsqrt(square / g.d + EPSILON))

    def last(i):
        rows = pl.ds(i * g.rb, g.rb)
        for k in range(g.strips):
            cols = pl.ds(k * 128, 128)
            v = T1[0, rows, cols].astype(F32) * SC[0, rows, :] * pgain[1:2, cols]
            out[rows, cols] = (X1[x, rows, cols].astype(F32) + v).astype(BF16)

    loop(last, 0, g.blocks)
    for copy in sent:
        copy.wait_send()


def local(g, tokens, pre_gain, w_value, w_gate, taps, norm_gain, norm_shift, w_out, post_gain):
    w_out = jnp.swapaxes(w_out, 1, 2)
    taps = jnp.swapaxes(taps, 0, 1)
    vm = pl.BlockSpec(memory_space=pltpu.VMEM)
    slots = (g.nz, g.ny, g.nc, 2, g.kr, g.ch)
    rows, ch = g.rows, g.ch
    most = max(g.ny, g.nz)
    dma = pltpu.SemaphoreType.DMA
    scratch = [
        pltpu.VMEM(slots, BF16),
        pltpu.VMEM(slots, BF16),
        pltpu.VMEM(slots, BF16),
        pltpu.VMEM((g.nx, rows, ch), BF16),
        pltpu.VMEM((g.nx, rows, ch), BF16),
        pltpu.VMEM((g.nx, rows, ch), BF16),
        pltpu.VMEM((g.nx, rows, ch), BF16),
        pltpu.VMEM((rows, ch), F32),
        pltpu.VMEM((rows, ch), F32),
        pltpu.VMEM((g.strips, HALO + rows, 128), F32),
        pltpu.VMEM((2, HALO, ch), BF16),
        pltpu.VMEM((2, HALO, ch), BF16),
        pltpu.VMEM((g.strips, rows, 128), F32),
        pltpu.VMEM((g.rp, 128), F32),
        pltpu.VMEM((g.rp, 128), F32),
        pltpu.VMEM((rows, ch), BF16),
        pltpu.VMEM((3, g.nx, 8, g.rp), F32),
        pltpu.VMEM((2, g.rp, 128), F32),
        pltpu.VMEM((g.nx, 8, ch), F32),
        pltpu.VMEM((2, rows, ch), BF16),
        pltpu.VMEM((2, 2, rows, ch), BF16),
        pltpu.VMEM((2, 2, rows // 2, ch), BF16),
        pltpu.VMEM((2, 2, rows, ch), BF16),
        pltpu.VMEM((rows, ch), F32),
        dma((4, 2, most)),
        dma((4, 2, most)),
        dma((6, 2, 2, most // 2)),
        dma((6, 2, 2, most // 2)),
        dma((4, 2, most)),
        dma((4, 2, most)),
        dma((2, 2, 3)),
        dma((2, 2, 3)),
        dma((2, 4)),
        dma((2, 4)),
        dma((3, 3)),
        dma((3, 3)),
        dma((3,)),
        dma((3,)),
        dma((2,)),
        dma((2,)),
    ]
    return pl.pallas_call(
        functools.partial(body, g),
        out_shape=jax.ShapeDtypeStruct((rows, ch), BF16),
        in_specs=[vm] * 9,
        out_specs=vm,
        scratch_shapes=scratch,
        compiler_params=pltpu.CompilerParams(
            collective_id=0, has_side_effects=True, vmem_limit_bytes=60 * 1024 * 1024
        ),
    )(tokens, pre_gain, w_value, w_gate, taps, norm_gain, norm_shift, w_out, post_gain)


def build(mesh, sizes, rows, ch, width):
    g = Geometry(*sizes, mesh.shape["tp"], rows, ch, width)
    placed = (
        P("sp", "tp"),
        P(),
        P(None, "sp", "tp"),
        P(None, "sp", "tp"),
        P(None, None, "tp"),
        P(None, "tp"),
        P(None, "tp"),
        P(None, "tp", "sp"),
        P(None, "tp"),
    )
    return jax.shard_map(
        functools.partial(local, g), mesh=mesh, in_specs=placed, out_specs=P("sp", "tp"), check_vma=False
    )


def solution(mesh):
    return build(mesh, (8, 8, 2), 320, 512, 31)
```

```python
import functools

import jax
import jax.numpy as jnp
from jax import lax
from jax.experimental import pallas as pl
from jax.experimental.pallas import tpu as pltpu
from jax.sharding import PartitionSpec as P

EPSILON = 1e-06
LN_EPSILON = 1e-05
HALO = 32
F32 = jnp.float32
BF16 = jnp.bfloat16
MESH = pl.DeviceIdType.MESH


class Geometry:
    def __init__(self, nz, ny, nc, nx, rows, ch, taps):
        self.nz, self.ny, self.nc, self.nx = nz, ny, nc, nx
        self.rows, self.ch, self.taps = rows, ch, taps
        self.d = ch * nx
        self.nsp = nz * ny * nc
        self.kr = self.d // self.nsp
        self.strips = ch // 128
        self.rb = 64
        self.blocks = rows // self.rb
        first = self.blocks - self.blocks // 2
        self.split = (self.blocks - first) * self.rb
        self.chunks = tuple((lo, n, -(-n // 128) * 128) for lo, n in ((self.split, rows - self.split), (0, self.split)))
        self.wide = max(w for _, _, w in self.chunks)


def body(
    g,
    tok, pre_gain, wv, wg, taps, ngain, nshift, wo, pgain,
    out,
    WV, WG, WO, X0, PJ, X1, NB, AV, AG, GF, FT, FR, CV, S1, S2, ACT, STB, SC, PG, T1, T2, R1, R2, OWN, PQ,
    esend, erecv, wsend, wrecv, dsend, drecv, asend, arecv, rsend, rrecv, ssend, srecv, gsend, grecv, fsend, frecv,
):
    s = lax.axis_index("sp")
    x = lax.axis_index("tp")
    c = lax.rem(s, g.nc)
    y = lax.rem(lax.div(s, g.nc), g.ny)
    z = lax.div(s, g.nc * g.ny)
    sgn = 1 - 2 * c

    def rows_of(q, part=None):
        lo, n, _ = g.chunks[q]
        if part is None:
            return pl.ds(lo, n)
        return pl.ds(lo + part * (n // 2), n // 2)

    def sp_of(zz, yy, cc):
        return (zz * g.ny + yy) * g.nc + cc

    def at_x(j):
        return lax.rem(x + j + g.nx, g.nx)

    def remote(src, dst, send, recv, sp=None, tp=None):
        return pltpu.make_async_remote_copy(
            src_ref=src, dst_ref=dst, send_sem=send, recv_sem=recv,
            device_id=(s if sp is None else sp, x if tp is None else tp),
            device_id_type=MESH,
        )

    sent = []

    def go(copy):
        copy.start()
        sent.append(copy)

    size = {"y": g.ny, "z": g.nz}
    here = {"y": y, "z": z}

    def moved(axis, by):
        n = size[axis]
        return lax.rem(here[axis] + by + 2 * n, n)

    def ring_sp(axis, by):
        p = moved(axis, by)
        return sp_of(z, p, c) if axis == "y" else sp_of(p, y, c)

    partner = sp_of(z, y, 1 - c)
    after = lax.rem(s + 1, g.nsp)
    before = lax.rem(s + g.nsp - 1, g.nsp)

    for layer in range(2):
        WV[z, y, c, layer] = wv[layer]
        WG[z, y, c, layer] = wg[layer]
        WO[z, y, c, layer] = wo[layer]
    PG[x] = jnp.broadcast_to(pgain[0:1, :], (8, g.ch))
    X0[x] = tok[...]
    STB[...] = jnp.zeros_like(STB)
    S1[...] = jnp.zeros_like(S1)
    S2[...] = jnp.zeros_like(S2)

    barrier = pltpu.get_barrier_semaphore()
    greet = [(None, at_x(j)) for j in range(1, g.nx)]
    greet += [(after, None), (before, None)]
    if g.nc > 1:
        greet.append((partner, None))
    for axis in ("y", "z"):
        greet += [(ring_sp(axis, k), None) for k in range(1, size[axis])]
    for sp, tp in greet:
        pl.semaphore_signal(
            barrier, inc=1,
            device_id=(s if sp is None else sp, x if tp is None else tp),
            device_id_type=MESH,
        )
    pl.semaphore_wait(barrier, len(greet))

    order = (("y", "z"), ("z", "y"))
    lanes = g.ch // 2
    pieces = {0: (0, 1), 1: (2,), 2: (3, 4), 3: (5,)}

    def source(item, stream):
        if item % 2 == 0:
            return (WV, WG)[stream], pl.ds(0, g.ch)
        return WO, pl.ds(stream * lanes, lanes)

    def own_slot(item, stream, pos):
        buf, cols = source(item, stream)
        zz, yy = (z, pos) if stream == 0 else (pos, y)
        return buf.at[zz, yy, c, item // 2, :, cols]

    def block(item, stream, pos, core, piece=None):
        buf, cols = source(item, stream)
        across_dim = slice(None)
        if piece is not None and len(pieces[item]) == 2:
            n = size[order[stream][0]] // 2
            near = lax.div(here[order[stream][0]], n)
            across_dim = pl.ds((near if piece == pieces[item][0] else 1 - near) * n, n)
        if stream == 0:
            return buf.at[pos, across_dim, core, item // 2, :, cols]
        return buf.at[across_dim, pos, core, item // 2, :, cols]

    def hops(axis):
        n = size[axis]
        return (n // 2, n - 1 - n // 2)

    def scatter_copy(item, stream, k):
        axis = order[stream][0]
        ref = own_slot(item, stream, here[axis])
        return remote(ref, ref, esend.at[item, stream, k], erecv.at[item, stream, k], sp=ring_sp(axis, k))

    def farthest_first(n):
        return sorted(range(1, n), key=lambda k: -min(k, n - k))

    def scatter(item):
        for k in farthest_first(max(g.ny, g.nz)):
            for stream in range(2):
                if k < size[order[stream][0]]:
                    go(scatter_copy(item, stream, k))

    def scattered(item):
        for stream in range(2):
            axis = order[stream][0]
            for k in range(1, size[axis]):
                ref = own_slot(item, stream, moved(axis, -k))
                remote(
                    ref, ref, esend.at[item, stream, k], erecv.at[item, stream, k], sp=ring_sp(axis, k)
                ).wait_recv()

    def ring_copy(item, piece, stream, way, step, back):
        axis = order[stream][1]
        toward = sgn if way == 0 else -sgn
        ref = block(item, stream, moved(axis, -toward * (step + back)), c, piece)
        return remote(
            ref, ref,
            wsend.at[piece, stream, way, step],
            wrecv.at[piece, stream, way, step],
            sp=ring_sp(axis, toward),
        )

    def across(item, stream, index, pos):
        if g.nc > 1:
            ref = block(item, stream, pos, c)
            go(remote(ref, ref, dsend.at[item, stream, index], drecv.at[item, stream, index], sp=partner))

    def begin(item):
        for piece in pieces[item]:
            for stream in range(2):
                axis = order[stream][1]
                for way in range(2):
                    if hops(axis)[way] > 0:
                        go(ring_copy(item, piece, stream, way, 0, 0))
        for stream in range(2):
            across(item, stream, 0, here[order[stream][1]])

    def advance(item, step):
        for piece in pieces[item]:
            for stream in range(2):
                axis = order[stream][1]
                for way in range(2):
                    if step < hops(axis)[way]:
                        ring_copy(item, piece, stream, way, step, 1).wait_recv()
                        if step + 1 < hops(axis)[way]:
                            go(ring_copy(item, piece, stream, way, step + 1, 0))
                        if piece == pieces[item][-1]:
                            toward = sgn if way == 0 else -sgn
                            across(
                                item, stream, 1 + way * hops(axis)[0] + step,
                                moved(axis, -toward * (step + 1)),
                            )

    def finish(item):
        if g.nc > 1:
            for stream in range(2):
                axis = order[stream][1]
                for index in range(size[axis]):
                    ref = block(item, stream, index, 1 - c)
                    remote(
                        ref, ref, dsend.at[item, stream, index], drecv.at[item, stream, index], sp=partner
                    ).wait_recv()

    steps = max(g.ny, g.nz) // 2

    def spread_copy(layer, q, buf, way, piece, back):
        toward = 1 - 2 * way
        origin = at_x(-toward * (back + (piece == 2)))
        ref = buf.at[origin, rows_of(q, 1 - way if piece == 1 else way)]
        return remote(
            ref, ref, asend.at[layer, q, way, piece], arecv.at[layer, q, way, piece], tp=at_x(toward)
        )

    def spread_begin(layer, q, buf):
        for piece in range(2):
            for way in range(2):
                go(spread_copy(layer, q, buf, way, piece, 0))

    def spread_relay(layer, q, buf):
        for way in range(2):
            spread_copy(layer, q, buf, way, 0, 1).wait_recv()
            go(spread_copy(layer, q, buf, way, 2, 0))

    def spread_end(layer, q, buf):
        for piece in (1, 2):
            for way in range(2):
                spread_copy(layer, q, buf, way, piece, 1).wait_recv()

    def tell(which):
        for j in range(1, g.nx):
            ref = STB.at[which, x]
            go(remote(ref, ref, ssend.at[which, j - 1], srecv.at[which, j - 1], tp=at_x(j)))

    def told(which):
        for j in range(1, g.nx):
            ref = STB.at[which, at_x(-j)]
            remote(ref, ref, ssend.at[which, j - 1], srecv.at[which, j - 1], tp=at_x(j)).wait_recv()

    def put_sums(which, row, buf, q):
        w = g.chunks[q][2]
        STB[which, x, row : row + 1, 0:w] = jnp.sum(jnp.transpose(buf[q, 0:w, :]), axis=0, keepdims=True)

    def as_columns(q, k, row):
        w = g.chunks[q][2]
        SC[q, k, 0:w, :] = jnp.transpose(jnp.broadcast_to(row, (128, w)))

    scatter(0)
    for q in range(2):
        spread_begin(0, q, X0)
    scatter(1)
    for j in range(1, g.nx):
        go(remote(PG.at[x], PG.at[x], gsend.at[j - 1], grecv.at[j - 1], tp=at_x(j)))
    scattered(0)
    begin(0)
    scattered(1)
    begin(1)
    scatter(2)
    scatter(3)
    for q in range(2):
        spread_relay(0, q, X0)
    advance(0, 0)
    advance(1, 0)
    for q in range(2):
        spread_end(0, q, X0)

    def loop(fn, lo, hi):
        def at(i, carry):
            fn(i)
            return carry

        lax.fori_loop(lo, hi, at, 0)

    def over(q, fn):
        lo, n, _ = g.chunks[q]
        loop(fn, lo // g.rb, (lo + n) // g.rb)

    def norm_rows(layer, i):
        rows = pl.ds(i * g.rb, g.rb)
        if layer == 1:
            square = jnp.zeros((g.rb, 1), F32)
            for j in range(g.nx):
                v = PJ[j, rows, :].astype(F32)
                square += jnp.sum(v * v, -1, keepdims=True)
            scale = lax.rsqrt(square / g.d + EPSILON)
        total = jnp.zeros((g.rb, 1), F32)
        for j in range(g.nx):
            v = X0[j, rows, :].astype(F32)
            if layer == 1:
                v = v + PJ[j, rows, :].astype(F32) * scale * PG[j, 0:1, :]
                X1[j, rows, :] = v.astype(BF16)
                v = v.astype(BF16).astype(F32)
            total += jnp.sum(v * v, -1, keepdims=True)
        inv = lax.rsqrt(total / g.d + EPSILON)
        for j in range(g.nx):
            v = (X0, X1)[layer][j, rows, :].astype(F32)
            cols = pl.ds(j * g.ch, g.ch)
            NB[j, rows, :] = (v * inv * pre_gain[layer : layer + 1, cols]).astype(BF16)

    zs = g.nz // g.nx

    def project_in(layer, rows):
        for acc, w in ((AV, WV), (AG, WG)):
            def term(j):
                mat = w[pl.ds(j * zs, zs), :, :, layer].reshape(g.ch, g.ch)
                return jnp.dot(NB[j, rows, :], mat, preferred_element_type=F32)

            def at(j, carry):
                acc[rows, :] += term(j)
                return carry

            acc[rows, :] = term(0)
            lax.fori_loop(1, g.nx, at, 0)

    def gate(i):
        rows = pl.ds(i * g.rb, g.rb)
        for k in range(g.strips):
            cols = pl.ds(k * 128, 128)
            act = (AV[rows, cols] * jax.nn.sigmoid(AG[rows, cols])).astype(BF16)
            GF[k, pl.ds(HALO + i * g.rb, g.rb), :] = act.astype(F32)

    def fringe_copy(layer):
        return remote(FT.at[layer], FR.at[layer], fsend.at[layer], frecv.at[layer], sp=after)

    def fringe_send(layer):
        for k in range(g.strips):
            FT[layer, :, k * 128 : (k + 1) * 128] = GF[k, g.rows : g.rows + HALO, :].astype(BF16)
        go(fringe_copy(layer))

    def fringe_take(layer):
        fringe_copy(layer).wait_recv()
        keep = jnp.where(s > 0, 1.0, 0.0).astype(F32)
        for k in range(g.strips):
            GF[k, 0:HALO, :] = FR[layer, :, k * 128 : (k + 1) * 128].astype(F32) * keep

    def convolve(layer, q, i):
        whole = [jnp.zeros((g.rb, 128), F32) for _ in range(2)]
        for k in range(g.strips):
            cols = pl.ds(k * 128, 128)
            acc = jnp.zeros((g.rb, 128), F32)
            for tap in range(g.taps):
                rows = pl.ds(i * g.rb + (HALO - g.taps + 1 + tap), g.rb)
                acc = acc + taps[tap, layer : layer + 1, cols] * GF[k, rows, :]
            CV[k, pl.ds(i * g.rb, g.rb), :] = acc
            whole = [whole[0] + acc, whole[1] + acc * acc]
        local_rows = pl.ds(i * g.rb - g.chunks[q][0], g.rb)
        S1[q, local_rows, :] = whole[0]
        S2[q, local_rows, :] = whole[1]

    def activate(layer, q, i):
        rows = pl.ds(i * g.rb, g.rb)
        local_rows = pl.ds(i * g.rb - g.chunks[q][0], g.rb)
        center = SC[q, 0, local_rows, :]
        inv = SC[q, 1, local_rows, :]
        for k in range(g.strips):
            cols = pl.ds(k * 128, 128)
            v = (CV[k, rows, :] - center) * inv * ngain[layer : layer + 1, cols] + nshift[
                layer : layer + 1, cols
            ]
            ACT[rows, cols] = (v * jax.nn.sigmoid(v)).astype(BF16)

    def stats_send(layer, q):
        put_sums(2 * layer + q, 0, S1, q)
        put_sums(2 * layer + q, 1, S2, q)
        tell(2 * layer + q)

    def stats_take(layer, q):
        which, w = 2 * layer + q, g.chunks[q][2]
        told(which)
        sums = STB[which, 0, :, 0:w]
        for j in range(1, g.nx):
            sums = sums + STB[which, j, :, 0:w]
        center = sums[0:1, :] / g.d
        spread = jnp.maximum(sums[1:2, :] / g.d - center * center, 0.0)
        as_columns(q, 0, center)
        as_columns(q, 1, lax.rsqrt(spread + LN_EPSILON))

    def part_for(layer, q, dest):
        mat = WO[pl.ds(dest * zs, zs), :, :, layer].reshape(g.ch, g.ch)
        return lax.dot_general(
            ACT[rows_of(q), :], mat, (((1,), (1,)), ((), ())), preferred_element_type=F32
        )

    def far_hop(layer, q, way):
        part = rows_of(q, way)
        return remote(
            T1.at[layer, part], R1.at[layer, way, part],
            rsend.at[layer, q, way], rrecv.at[layer, q, way], tp=at_x(1 - 2 * way),
        )

    def near_hop(layer, q, way, added):
        part = rows_of(q, way if added else 1 - way)
        index = 2 + 2 * way + added
        return remote(
            T2.at[layer, way, part], R2.at[layer, way, part],
            rsend.at[layer, q, index], rrecv.at[layer, q, index], tp=at_x(1 - 2 * way),
        )

    def shares(layer, q):
        T1[layer, rows_of(q)] = part_for(layer, q, at_x(2)).astype(BF16)
        for way in range(2):
            go(far_hop(layer, q, way))
        for way in range(2):
            OWN[way, rows_of(q)] = part_for(layer, q, at_x(1 - 2 * way))
            part = rows_of(q, 1 - way)
            T2[layer, way, part] = OWN[way, part].astype(BF16)
            go(near_hop(layer, q, way, 0))

    def relay_shares(layer, q):
        for way in range(2):
            far_hop(layer, q, way).wait_recv()
            part = rows_of(q, way)
            T2[layer, way, part] = (OWN[way, part] + R1[layer, way, part].astype(F32)).astype(BF16)
            go(near_hop(layer, q, way, 1))

    def own_share(layer, q):
        OWN[2, rows_of(q)] = part_for(layer, q, x)

    def shares_end(layer, q):
        for added in range(2):
            for way in range(2):
                near_hop(layer, q, way, added).wait_recv()

        def combine(i):
            rows = pl.ds(i * g.rb, g.rb)
            v = (OWN[2, rows] + R2[layer, 0, rows].astype(F32) + R2[layer, 1, rows].astype(F32)).astype(BF16)
            if layer == 0:
                PJ[x, rows, :] = v
            else:
                PQ[rows, :] = v
                v = v.astype(F32)
                v = v * v
                S1[q, pl.ds(i * g.rb - g.chunks[q][0], g.rb), :] = sum(
                    v[:, k * 128 : (k + 1) * 128] for k in range(g.strips)
                )

        over(q, combine)

    A, B = 0, 1
    for layer in range(2):
        if layer == 0:
            loop(lambda i: norm_rows(0, i), 0, g.blocks)
            for step in range(1, steps):
                advance(0, step)
                advance(1, step)
            scattered(2)
            begin(2)
            scattered(3)
            begin(3)
            finish(0)
            project_in(0, pl.ds(0, g.rows))
            finish(1)
            over(A, gate)
            fringe_send(0)
            over(B, gate)
        else:
            spread_end(1, A, PJ)
            over(A, lambda i: norm_rows(1, i))
            finish(2)
            project_in(1, rows_of(A))
            over(A, gate)
            fringe_send(1)
            spread_end(1, B, PJ)
            over(B, lambda i: norm_rows(1, i))
            project_in(1, rows_of(B))
            over(B, gate)
            finish(3)
        over(A, lambda i: convolve(layer, A, i))
        stats_send(layer, A)
        loop(lambda i: convolve(layer, B, i), 1, g.split // g.rb)
        fringe_take(layer)
        loop(lambda i: convolve(layer, B, i), 0, 1)
        stats_send(layer, B)
        if layer == 0:
            advance(2, 0)
            advance(3, 0)
        stats_take(layer, A)
        over(A, lambda i: activate(layer, A, i))
        shares(layer, A)
        stats_take(layer, B)
        over(B, lambda i: activate(layer, B, i))
        shares(layer, B)
        relay_shares(layer, A)
        if layer == 0:
            advance(2, 1)
            advance(3, 1)
        own_share(layer, A)
        relay_shares(layer, B)
        own_share(layer, B)
        for q in (A, B):
            shares_end(layer, q)
            if layer == 0:
                spread_begin(1, q, PJ)
                advance(2, 2 + q)
                advance(3, 2 + q)
            else:
                put_sums(4 + q, 0, S1, q)
                tell(4 + q)
        if layer == 0:
            for j in range(1, g.nx):
                ref = PG.at[at_x(-j)]
                remote(ref, ref, gsend.at[j - 1], grecv.at[j - 1], tp=at_x(j)).wait_recv()
            for q in (A, B):
                spread_relay(1, q, PJ)

    for q in (A, B):
        told(4 + q)
        square = sum(STB[4 + q, j, 0:1, 0 : g.chunks[q][2]] for j in range(g.nx))
        as_columns(q, 0, lax.rsqrt(square / g.d + EPSILON))

        def last(i):
            rows = pl.ds(i * g.rb, g.rb)
            scale = SC[q, 0, pl.ds(i * g.rb - g.chunks[q][0], g.rb), :]
            for k in range(g.strips):
                cols = pl.ds(k * 128, 128)
                v = PQ[rows, cols].astype(F32) * scale * pgain[1:2, cols]
                out[rows, cols] = (X1[x, rows, cols].astype(F32) + v).astype(BF16)

        over(q, last)
    for copy in sent:
        copy.wait_send()


def local(g, tokens, pre_gain, w_value, w_gate, taps, norm_gain, norm_shift, w_out, post_gain):
    w_out = jnp.swapaxes(w_out, 1, 2)
    taps = jnp.swapaxes(taps, 0, 1)
    vm = pl.BlockSpec(memory_space=pltpu.VMEM)
    slots = (g.nz, g.ny, g.nc, 2, g.kr, g.ch)
    rows, ch = g.rows, g.ch
    most = max(g.ny, g.nz)
    dma = pltpu.SemaphoreType.DMA
    scratch = [
        pltpu.VMEM(slots, BF16),
        pltpu.VMEM(slots, BF16),
        pltpu.VMEM(slots, BF16),
        pltpu.VMEM((g.nx, rows, ch), BF16),
        pltpu.VMEM((g.nx, rows, ch), BF16),
        pltpu.VMEM((g.nx, rows, ch), BF16),
        pltpu.VMEM((g.nx, rows, ch), BF16),
        pltpu.VMEM((rows, ch), F32),
        pltpu.VMEM((rows, ch), F32),
        pltpu.VMEM((g.strips, HALO + rows, 128), F32),
        pltpu.VMEM((2, HALO, ch), BF16),
        pltpu.VMEM((2, HALO, ch), BF16),
        pltpu.VMEM((g.strips, rows, 128), F32),
        pltpu.VMEM((2, g.wide, 128), F32),
        pltpu.VMEM((2, g.wide, 128), F32),
        pltpu.VMEM((rows, ch), BF16),
        pltpu.VMEM((6, g.nx, 8, g.wide), F32),
        pltpu.VMEM((2, 2, g.wide, 128), F32),
        pltpu.VMEM((g.nx, 8, ch), F32),
        pltpu.VMEM((2, rows, ch), BF16),
        pltpu.VMEM((2, 2, rows, ch), BF16),
        pltpu.VMEM((2, 2, rows, ch), BF16),
        pltpu.VMEM((2, 2, rows, ch), BF16),
        pltpu.VMEM((3, rows, ch), F32),
        pltpu.VMEM((rows, ch), BF16),
        dma((4, 2, most)),
        dma((4, 2, most)),
        dma((6, 2, 2, most // 2)),
        dma((6, 2, 2, most // 2)),
        dma((4, 2, most)),
        dma((4, 2, most)),
        dma((2, 2, 2, 3)),
        dma((2, 2, 2, 3)),
        dma((2, 2, 6)),
        dma((2, 2, 6)),
        dma((6, 3)),
        dma((6, 3)),
        dma((3,)),
        dma((3,)),
        dma((2,)),
        dma((2,)),
    ]
    return pl.pallas_call(
        functools.partial(body, g),
        out_shape=jax.ShapeDtypeStruct((rows, ch), BF16),
        in_specs=[vm] * 9,
        out_specs=vm,
        scratch_shapes=scratch,
        compiler_params=pltpu.CompilerParams(
            collective_id=0, has_side_effects=True, vmem_limit_bytes=60 * 1024 * 1024
        ),
    )(tokens, pre_gain, w_value, w_gate, taps, norm_gain, norm_shift, w_out, post_gain)


def build(mesh, sizes, rows, ch, width):
    g = Geometry(*sizes, mesh.shape["tp"], rows, ch, width)
    placed = (
        P("sp", "tp"),
        P(),
        P(None, "sp", "tp"),
        P(None, "sp", "tp"),
        P(None, None, "tp"),
        P(None, "tp"),
        P(None, "tp"),
        P(None, "tp", "sp"),
        P(None, "tp"),
    )
    return jax.shard_map(
        functools.partial(local, g), mesh=mesh, in_specs=placed, out_specs=P("sp", "tp"), check_vma=False
    )


def solution(mesh):
    return build(mesh, (8, 8, 2), 320, 512, 31)
```

```python
import functools

import jax
import jax.numpy as jnp
from jax import lax
from jax.experimental import pallas as pl
from jax.experimental.pallas import tpu as pltpu
from jax.sharding import PartitionSpec as P

EPSILON = 1e-06
LN_EPSILON = 1e-05
HALO = 32
F32 = jnp.float32
BF16 = jnp.bfloat16
MESH = pl.DeviceIdType.MESH


class Geometry:
    def __init__(self, nz, ny, nc, nx, rows, ch, taps):
        self.nz, self.ny, self.nc, self.nx = nz, ny, nc, nx
        self.rows, self.ch, self.taps = rows, ch, taps
        self.d = ch * nx
        self.nsp = nz * ny * nc
        self.kr = self.d // self.nsp
        self.strips = ch // 128
        self.rb = 64
        self.blocks = rows // self.rb
        first = self.blocks // 2
        self.split = (self.blocks - first) * self.rb
        self.chunks = tuple((lo, n, -(-n // 128) * 128) for lo, n in ((self.split, rows - self.split), (0, self.split)))
        self.wide = max(w for _, _, w in self.chunks)


def body(
    g,
    tok, pre_gain, wv, wg, taps, ngain, nshift, wo, pgain,
    out,
    WV, WG, WO, X0, PJ, X1, NB, AV, AG, GF, FT, FR, CV, S1, S2, ACT, STB, SC, PG, T1, T2, R1, R2, OWN, PQ,
    esend, erecv, wsend, wrecv, dsend, drecv, asend, arecv, rsend, rrecv, ssend, srecv, gsend, grecv, fsend, frecv,
):
    s = lax.axis_index("sp")
    x = lax.axis_index("tp")
    c = lax.rem(s, g.nc)
    y = lax.rem(lax.div(s, g.nc), g.ny)
    z = lax.div(s, g.nc * g.ny)
    sgn = 1 - 2 * c

    def rows_of(q, part=None):
        lo, n, _ = g.chunks[q]
        if part is None:
            return pl.ds(lo, n)
        return pl.ds(lo + part * (n // 2), n // 2)

    def sp_of(zz, yy, cc):
        return (zz * g.ny + yy) * g.nc + cc

    def at_x(j):
        return lax.rem(x + j + g.nx, g.nx)

    def remote(src, dst, send, recv, sp=None, tp=None):
        return pltpu.make_async_remote_copy(
            src_ref=src, dst_ref=dst, send_sem=send, recv_sem=recv,
            device_id=(s if sp is None else sp, x if tp is None else tp),
            device_id_type=MESH,
        )

    sent = []

    def go(copy):
        copy.start()
        sent.append(copy)

    size = {"y": g.ny, "z": g.nz}
    here = {"y": y, "z": z}

    def moved(axis, by):
        n = size[axis]
        return lax.rem(here[axis] + by + 2 * n, n)

    def ring_sp(axis, by):
        p = moved(axis, by)
        return sp_of(z, p, c) if axis == "y" else sp_of(p, y, c)

    partner = sp_of(z, y, 1 - c)
    after = lax.rem(s + 1, g.nsp)
    before = lax.rem(s + g.nsp - 1, g.nsp)

    for layer in range(2):
        WV[z, y, c, layer] = wv[layer]
        WG[z, y, c, layer] = wg[layer]
        WO[z, y, c, layer] = wo[layer]
    PG[x] = jnp.broadcast_to(pgain[0:1, :], (8, g.ch))
    X0[x] = tok[...]
    STB[...] = jnp.zeros_like(STB)
    S1[...] = jnp.zeros_like(S1)
    S2[...] = jnp.zeros_like(S2)

    barrier = pltpu.get_barrier_semaphore()
    greet = [(None, at_x(j)) for j in range(1, g.nx)]
    greet += [(after, None), (before, None)]
    if g.nc > 1:
        greet.append((partner, None))
    for axis in ("y", "z"):
        greet += [(ring_sp(axis, k), None) for k in range(1, size[axis])]
    for sp, tp in greet:
        pl.semaphore_signal(
            barrier, inc=1,
            device_id=(s if sp is None else sp, x if tp is None else tp),
            device_id_type=MESH,
        )
    pl.semaphore_wait(barrier, len(greet))

    order = (("y", "z"), ("z", "y"))
    lanes = g.ch // 2
    pieces = {0: (0, 1), 1: (2,), 2: (3,), 3: (4,)}

    def source(item, stream):
        if item % 2 == 0:
            return (WV, WG)[stream], pl.ds(0, g.ch)
        return WO, pl.ds(stream * lanes, lanes)

    def own_slot(item, stream, pos):
        buf, cols = source(item, stream)
        zz, yy = (z, pos) if stream == 0 else (pos, y)
        return buf.at[zz, yy, c, item // 2, :, cols]

    def block(item, stream, pos, core, piece=None):
        buf, cols = source(item, stream)
        across_dim = slice(None)
        if piece is not None and len(pieces[item]) == 2:
            n = size[order[stream][0]] // 2
            near = lax.div(here[order[stream][0]], n)
            across_dim = pl.ds((near if piece == pieces[item][0] else 1 - near) * n, n)
        if stream == 0:
            return buf.at[pos, across_dim, core, item // 2, :, cols]
        return buf.at[across_dim, pos, core, item // 2, :, cols]

    def hops(axis):
        n = size[axis]
        return (n // 2, n - 1 - n // 2)

    def scatter_copy(item, stream, k):
        axis = order[stream][0]
        if k == 0:
            buf, cols = source(item, stream)
            some = pl.ds(0, size[axis] - 1)
            zz, yy = (z, some) if stream == 0 else (some, y)
            ref = buf.at[zz, yy, c, item // 2, :, cols]
        else:
            ref = own_slot(item, stream, here[axis])
        return remote(ref, ref, esend.at[item, stream], erecv.at[item, stream], sp=ring_sp(axis, max(k, 1)))

    def farthest_first(n):
        return sorted(range(1, n), key=lambda k: -min(k, n - k))

    def scatter(item):
        for k in farthest_first(max(g.ny, g.nz)):
            for stream in range(2):
                if k < size[order[stream][0]]:
                    scatter_copy(item, stream, k).start()
        for stream in range(2):
            if size[order[stream][0]] > 1:
                sent.append(scatter_copy(item, stream, 0))

    def scattered(item):
        for stream in range(2):
            if size[order[stream][0]] > 1:
                scatter_copy(item, stream, 0).wait_recv()

    def ring_copy(item, piece, stream, way, step, back):
        axis = order[stream][1]
        toward = sgn if way == 0 else -sgn
        ref = block(item, stream, moved(axis, -toward * (step + back)), c, piece)
        return remote(
            ref, ref,
            wsend.at[piece, stream],
            wrecv.at[piece, stream, way, step],
            sp=ring_sp(axis, toward),
        )

    def ring_sent(item, piece, stream):
        buf, cols = source(item, stream)
        first, second = (size[axis] for axis in order[stream])
        one, some = pl.ds(0, first // len(pieces[item])), pl.ds(0, second - 1)
        zz, yy = (some, one) if stream == 0 else (one, some)
        ref = buf.at[zz, yy, c, item // 2, :, cols]
        return remote(ref, ref, wsend.at[piece, stream], wrecv.at[piece, stream, 0, 0], sp=partner)

    def across(item, stream, pos=None):
        if pos is None:
            buf, cols = source(item, stream)
            ref = buf.at[:, :, c, item // 2, :, cols]
        else:
            ref = block(item, stream, pos, c)
        return remote(ref, ref, dsend.at[item, stream], drecv.at[item, stream], sp=partner)

    def begin(item):
        for piece in pieces[item]:
            for stream in range(2):
                axis = order[stream][1]
                for way in range(2):
                    if hops(axis)[way] > 0:
                        ring_copy(item, piece, stream, way, 0, 0).start()
                if size[axis] > 1:
                    sent.append(ring_sent(item, piece, stream))
        if g.nc > 1 and item < 2:
            for stream in range(2):
                across(item, stream, here[order[stream][1]]).start()

    def advance(item, step):
        for piece in pieces[item]:
            for stream in range(2):
                axis = order[stream][1]
                for way in range(2):
                    if step < hops(axis)[way]:
                        ring_copy(item, piece, stream, way, step, 1).wait_recv()
                        if step + 1 < hops(axis)[way]:
                            ring_copy(item, piece, stream, way, step + 1, 0).start()
                        if g.nc > 1 and item < 2 and piece == pieces[item][-1]:
                            toward = sgn if way == 0 else -sgn
                            across(item, stream, moved(axis, -toward * (step + 1))).start()
        if step == steps - 1 and g.nc > 1:
            for stream in range(2):
                if item >= 2:
                    across(item, stream).start()
                sent.append(across(item, stream))

    def finish(item):
        if g.nc > 1:
            for stream in range(2):
                buf, cols = source(item, stream)
                ref = buf.at[:, :, 1 - c, item // 2, :, cols]
                remote(ref, ref, dsend.at[item, stream], drecv.at[item, stream], sp=partner).wait_recv()

    steps = max(g.ny, g.nz) // 2

    def spread_copy(layer, q, buf, way, piece, back):
        toward = 1 - 2 * way
        origin = at_x(-toward * (back + (piece == 2)))
        ref = buf.at[origin, rows_of(q, 1 - way if piece == 1 else way)]
        return remote(
            ref, ref, asend.at[layer, q, way, piece], arecv.at[layer, q, way, piece], tp=at_x(toward)
        )

    def spread_begin(layer, q, buf):
        for piece in range(2):
            for way in range(2):
                go(spread_copy(layer, q, buf, way, piece, 0))

    def spread_relay(layer, q, buf):
        for way in range(2):
            spread_copy(layer, q, buf, way, 0, 1).wait_recv()
            go(spread_copy(layer, q, buf, way, 2, 0))

    def spread_end(layer, q, buf):
        for piece in (1, 2):
            for way in range(2):
                spread_copy(layer, q, buf, way, piece, 1).wait_recv()

    def tell(which):
        for j in range(1, g.nx):
            ref = STB.at[which, x]
            go(remote(ref, ref, ssend.at[which, j - 1], srecv.at[which, j - 1], tp=at_x(j)))

    def told(which):
        for j in range(1, g.nx):
            ref = STB.at[which, at_x(-j)]
            remote(ref, ref, ssend.at[which, j - 1], srecv.at[which, j - 1], tp=at_x(j)).wait_recv()

    def put_sums(which, row, buf, q):
        w = g.chunks[q][2]
        STB[which, x, row : row + 1, 0:w] = jnp.sum(jnp.transpose(buf[q, 0:w, :]), axis=0, keepdims=True)

    def as_columns(q, k, row):
        w = g.chunks[q][2]
        SC[q, k, 0:w, :] = jnp.transpose(jnp.broadcast_to(row, (128, w)))

    scatter(0)
    for q in range(2):
        spread_begin(0, q, X0)
    scatter(1)
    for j in range(1, g.nx):
        go(remote(PG.at[x], PG.at[x], gsend.at[j - 1], grecv.at[j - 1], tp=at_x(j)))
    scattered(0)
    begin(0)
    scattered(1)
    begin(1)
    scatter(2)
    scatter(3)
    for q in range(2):
        spread_relay(0, q, X0)
    advance(0, 0)
    advance(1, 0)
    for q in range(2):
        spread_end(0, q, X0)

    def loop(fn, lo, hi):
        def at(i, carry):
            fn(i)
            return carry

        lax.fori_loop(lo, hi, at, 0)

    def over(q, fn):
        lo, n, _ = g.chunks[q]
        loop(fn, lo // g.rb, (lo + n) // g.rb)

    def norm_rows(layer, i):
        rows = pl.ds(i * g.rb, g.rb)
        if layer == 1:
            square = jnp.zeros((g.rb, 1), F32)
            for j in range(g.nx):
                v = PJ[j, rows, :].astype(F32)
                square += jnp.sum(v * v, -1, keepdims=True)
            scale = lax.rsqrt(square / g.d + EPSILON)
        total = jnp.zeros((g.rb, 1), F32)
        for j in range(g.nx):
            v = X0[j, rows, :].astype(F32)
            if layer == 1:
                v = v + PJ[j, rows, :].astype(F32) * scale * PG[j, 0:1, :]
                X1[j, rows, :] = v.astype(BF16)
                v = v.astype(BF16).astype(F32)
            total += jnp.sum(v * v, -1, keepdims=True)
        inv = lax.rsqrt(total / g.d + EPSILON)
        for j in range(g.nx):
            v = (X0, X1)[layer][j, rows, :].astype(F32)
            cols = pl.ds(j * g.ch, g.ch)
            NB[j, rows, :] = (v * inv * pre_gain[layer : layer + 1, cols]).astype(BF16)

    zs = g.nz // g.nx

    def project_in(layer, rows):
        for acc, w in ((AV, WV), (AG, WG)):
            def term(j):
                mat = w[pl.ds(j * zs, zs), :, :, layer].reshape(g.ch, g.ch)
                return jnp.dot(NB[j, rows, :], mat, preferred_element_type=F32)

            def at(j, carry):
                acc[rows, :] += term(j)
                return carry

            acc[rows, :] = term(0)
            lax.fori_loop(1, g.nx, at, 0)

    def gate(i):
        rows = pl.ds(i * g.rb, g.rb)
        for k in range(g.strips):
            cols = pl.ds(k * 128, 128)
            act = (AV[rows, cols] * jax.nn.sigmoid(AG[rows, cols])).astype(BF16)
            GF[k, pl.ds(HALO + i * g.rb, g.rb), :] = act.astype(F32)

    def fringe_copy(layer):
        return remote(FT.at[layer], FR.at[layer], fsend.at[layer], frecv.at[layer], sp=after)

    def fringe_send(layer):
        for k in range(g.strips):
            FT[layer, :, k * 128 : (k + 1) * 128] = GF[k, g.rows : g.rows + HALO, :].astype(BF16)
        go(fringe_copy(layer))

    def fringe_take(layer):
        fringe_copy(layer).wait_recv()
        keep = jnp.where(s > 0, 1.0, 0.0).astype(F32)
        for k in range(g.strips):
            GF[k, 0:HALO, :] = FR[layer, :, k * 128 : (k + 1) * 128].astype(F32) * keep

    def convolve(layer, q, i):
        whole = [jnp.zeros((g.rb, 128), F32) for _ in range(2)]
        for k in range(g.strips):
            cols = pl.ds(k * 128, 128)
            acc = jnp.zeros((g.rb, 128), F32)
            for tap in range(g.taps):
                rows = pl.ds(i * g.rb + (HALO - g.taps + 1 + tap), g.rb)
                acc = acc + taps[tap, layer : layer + 1, cols] * GF[k, rows, :]
            CV[k, pl.ds(i * g.rb, g.rb), :] = acc
            whole = [whole[0] + acc, whole[1] + acc * acc]
        local_rows = pl.ds(i * g.rb - g.chunks[q][0], g.rb)
        S1[q, local_rows, :] = whole[0]
        S2[q, local_rows, :] = whole[1]

    def activate(layer, q, i):
        rows = pl.ds(i * g.rb, g.rb)
        local_rows = pl.ds(i * g.rb - g.chunks[q][0], g.rb)
        center = SC[q, 0, local_rows, :]
        inv = SC[q, 1, local_rows, :]
        for k in range(g.strips):
            cols = pl.ds(k * 128, 128)
            v = (CV[k, rows, :] - center) * inv * ngain[layer : layer + 1, cols] + nshift[
                layer : layer + 1, cols
            ]
            ACT[rows, cols] = (v * jax.nn.sigmoid(v)).astype(BF16)

    def stats_send(layer, q):
        put_sums(2 * layer + q, 0, S1, q)
        put_sums(2 * layer + q, 1, S2, q)
        tell(2 * layer + q)

    def stats_take(layer, q):
        which, w = 2 * layer + q, g.chunks[q][2]
        told(which)
        sums = STB[which, 0, :, 0:w]
        for j in range(1, g.nx):
            sums = sums + STB[which, j, :, 0:w]
        center = sums[0:1, :] / g.d
        spread = jnp.maximum(sums[1:2, :] / g.d - center * center, 0.0)
        as_columns(q, 0, center)
        as_columns(q, 1, lax.rsqrt(spread + LN_EPSILON))

    def part_for(layer, q, dest):
        mat = WO[pl.ds(dest * zs, zs), :, :, layer].reshape(g.ch, g.ch)
        return lax.dot_general(
            ACT[rows_of(q), :], mat, (((1,), (1,)), ((), ())), preferred_element_type=F32
        )

    def far_hop(layer, q, way):
        part = rows_of(q, way)
        return remote(
            T1.at[layer, part], R1.at[layer, way, part],
            rsend.at[layer, q, way], rrecv.at[layer, q, way], tp=at_x(1 - 2 * way),
        )

    def near_hop(layer, q, way, added):
        part = rows_of(q, way if added else 1 - way)
        index = 2 + 2 * way + added
        return remote(
            T2.at[layer, way, part], R2.at[layer, way, part],
            rsend.at[layer, q, index], rrecv.at[layer, q, index], tp=at_x(1 - 2 * way),
        )

    def shares(layer, q):
        T1[layer, rows_of(q)] = part_for(layer, q, at_x(2)).astype(BF16)
        for way in range(2):
            go(far_hop(layer, q, way))
        for way in range(2):
            OWN[way, rows_of(q)] = part_for(layer, q, at_x(1 - 2 * way))
            part = rows_of(q, 1 - way)
            T2[layer, way, part] = OWN[way, part].astype(BF16)
            go(near_hop(layer, q, way, 0))

    def relay_shares(layer, q):
        for way in range(2):
            far_hop(layer, q, way).wait_recv()
            part = rows_of(q, way)
            T2[layer, way, part] = (OWN[way, part] + R1[layer, way, part].astype(F32)).astype(BF16)
            go(near_hop(layer, q, way, 1))

    def own_share(layer, q):
        OWN[2, rows_of(q)] = part_for(layer, q, x)

    def shares_end(layer, q):
        for added in range(2):
            for way in range(2):
                near_hop(layer, q, way, added).wait_recv()

        def combine(i):
            rows = pl.ds(i * g.rb, g.rb)
            v = (OWN[2, rows] + R2[layer, 0, rows].astype(F32) + R2[layer, 1, rows].astype(F32)).astype(BF16)
            if layer == 0:
                PJ[x, rows, :] = v
            else:
                PQ[rows, :] = v
                v = v.astype(F32)
                v = v * v
                S1[q, pl.ds(i * g.rb - g.chunks[q][0], g.rb), :] = sum(
                    v[:, k * 128 : (k + 1) * 128] for k in range(g.strips)
                )

        over(q, combine)

    A, B = 0, 1
    for layer in range(2):
        if layer == 0:
            loop(lambda i: norm_rows(0, i), 0, g.blocks)
            for step in range(1, steps):
                advance(0, step)
                advance(1, step)
            scattered(2)
            begin(2)
            scattered(3)
            begin(3)
            finish(0)
            project_in(0, pl.ds(0, g.rows))
            finish(1)
            over(A, gate)
            fringe_send(0)
            over(B, gate)
        else:
            spread_end(1, A, PJ)
            over(A, lambda i: norm_rows(1, i))
            finish(2)
            project_in(1, rows_of(A))
            over(A, gate)
            fringe_send(1)
            spread_end(1, B, PJ)
            over(B, lambda i: norm_rows(1, i))
            project_in(1, rows_of(B))
            over(B, gate)
            finish(3)
        over(A, lambda i: convolve(layer, A, i))
        stats_send(layer, A)
        loop(lambda i: convolve(layer, B, i), 1, g.split // g.rb)
        fringe_take(layer)
        loop(lambda i: convolve(layer, B, i), 0, 1)
        stats_send(layer, B)
        if layer == 0:
            advance(2, 0)
            advance(3, 0)
        stats_take(layer, A)
        over(A, lambda i: activate(layer, A, i))
        shares(layer, A)
        stats_take(layer, B)
        over(B, lambda i: activate(layer, B, i))
        shares(layer, B)
        relay_shares(layer, A)
        if layer == 0:
            advance(2, 1)
            advance(3, 1)
        own_share(layer, A)
        relay_shares(layer, B)
        own_share(layer, B)
        for q in (A, B):
            shares_end(layer, q)
            if layer == 0:
                spread_begin(1, q, PJ)
                advance(2, 2 + q)
                advance(3, 2 + q)
            else:
                put_sums(4 + q, 0, S1, q)
                tell(4 + q)
        if layer == 0:
            for j in range(1, g.nx):
                ref = PG.at[at_x(-j)]
                remote(ref, ref, gsend.at[j - 1], grecv.at[j - 1], tp=at_x(j)).wait_recv()
            for q in (A, B):
                spread_relay(1, q, PJ)

    for q in (A, B):
        told(4 + q)
        square = sum(STB[4 + q, j, 0:1, 0 : g.chunks[q][2]] for j in range(g.nx))
        as_columns(q, 0, lax.rsqrt(square / g.d + EPSILON))

        def last(i):
            rows = pl.ds(i * g.rb, g.rb)
            scale = SC[q, 0, pl.ds(i * g.rb - g.chunks[q][0], g.rb), :]
            for k in range(g.strips):
                cols = pl.ds(k * 128, 128)
                v = PQ[rows, cols].astype(F32) * scale * pgain[1:2, cols]
                out[rows, cols] = (X1[x, rows, cols].astype(F32) + v).astype(BF16)

        over(q, last)
    for copy in sent:
        copy.wait_send()


def local(g, tokens, pre_gain, w_value, w_gate, taps, norm_gain, norm_shift, w_out, post_gain):
    w_out = jnp.swapaxes(w_out, 1, 2)
    taps = jnp.swapaxes(taps, 0, 1)
    vm = pl.BlockSpec(memory_space=pltpu.VMEM)
    slots = (g.nz, g.ny, g.nc, 2, g.kr, g.ch)
    rows, ch = g.rows, g.ch
    most = max(g.ny, g.nz)
    dma = pltpu.SemaphoreType.DMA
    scratch = [
        pltpu.VMEM(slots, BF16),
        pltpu.VMEM(slots, BF16),
        pltpu.VMEM(slots, BF16),
        pltpu.VMEM((g.nx, rows, ch), BF16),
        pltpu.VMEM((g.nx, rows, ch), BF16),
        pltpu.VMEM((g.nx, rows, ch), BF16),
        pltpu.VMEM((g.nx, rows, ch), BF16),
        pltpu.VMEM((rows, ch), F32),
        pltpu.VMEM((rows, ch), F32),
        pltpu.VMEM((g.strips, HALO + rows, 128), F32),
        pltpu.VMEM((2, HALO, ch), BF16),
        pltpu.VMEM((2, HALO, ch), BF16),
        pltpu.VMEM((g.strips, rows, 128), F32),
        pltpu.VMEM((2, g.wide, 128), F32),
        pltpu.VMEM((2, g.wide, 128), F32),
        pltpu.VMEM((rows, ch), BF16),
        pltpu.VMEM((6, g.nx, 8, g.wide), F32),
        pltpu.VMEM((2, 2, g.wide, 128), F32),
        pltpu.VMEM((g.nx, 8, ch), F32),
        pltpu.VMEM((2, rows, ch), BF16),
        pltpu.VMEM((2, 2, rows, ch), BF16),
        pltpu.VMEM((2, 2, rows, ch), BF16),
        pltpu.VMEM((2, 2, rows, ch), BF16),
        pltpu.VMEM((3, rows, ch), F32),
        pltpu.VMEM((rows, ch), BF16),
        dma((4, 2)),
        dma((4, 2)),
        dma((5, 2)),
        dma((5, 2, 2, most // 2)),
        dma((4, 2)),
        dma((4, 2)),
        dma((2, 2, 2, 3)),
        dma((2, 2, 2, 3)),
        dma((2, 2, 6)),
        dma((2, 2, 6)),
        dma((6, 3)),
        dma((6, 3)),
        dma((3,)),
        dma((3,)),
        dma((2,)),
        dma((2,)),
    ]
    return pl.pallas_call(
        functools.partial(body, g),
        out_shape=jax.ShapeDtypeStruct((rows, ch), BF16),
        in_specs=[vm] * 9,
        out_specs=vm,
        scratch_shapes=scratch,
        compiler_params=pltpu.CompilerParams(
            collective_id=0, has_side_effects=True, vmem_limit_bytes=60 * 1024 * 1024
        ),
    )(tokens, pre_gain, w_value, w_gate, taps, norm_gain, norm_shift, w_out, post_gain)


def build(mesh, sizes, rows, ch, width):
    g = Geometry(*sizes, mesh.shape["tp"], rows, ch, width)
    placed = (
        P("sp", "tp"),
        P(),
        P(None, "sp", "tp"),
        P(None, "sp", "tp"),
        P(None, None, "tp"),
        P(None, "tp"),
        P(None, "tp"),
        P(None, "tp", "sp"),
        P(None, "tp"),
    )
    return jax.shard_map(
        functools.partial(local, g), mesh=mesh, in_specs=placed, out_specs=P("sp", "tp"), check_vma=False
    )


def solution(mesh):
    return build(mesh, (8, 8, 2), 320, 512, 31)
```

```python
import functools

import jax
import jax.numpy as jnp
from jax import lax
from jax.experimental import pallas as pl
from jax.experimental.pallas import tpu as pltpu
from jax.sharding import PartitionSpec as P

EPSILON = 1e-06
LN_EPSILON = 1e-05
HALO = 32
F32 = jnp.float32
BF16 = jnp.bfloat16
MESH = pl.DeviceIdType.MESH


class Geometry:
    def __init__(self, nz, ny, nc, nx, rows, ch, taps):
        self.nz, self.ny, self.nc, self.nx = nz, ny, nc, nx
        self.rows, self.ch, self.taps = rows, ch, taps
        self.d = ch * nx
        self.nsp = nz * ny * nc
        self.kr = self.d // self.nsp
        self.strips = ch // 128
        self.rb = 64
        self.blocks = rows // self.rb
        first = self.blocks // 2
        self.split = (self.blocks - first) * self.rb
        self.chunks = tuple((lo, n, -(-n // 128) * 128) for lo, n in ((self.split, rows - self.split), (0, self.split)))
        self.wide = max(w for _, _, w in self.chunks)


def body(
    g,
    tok, pre_gain, wv, wg, hbm_taps, ngain, nshift, wo, pgain,
    out,
    WV, WG, WO, X0, PJ, X1, NB, AV, AG, GF, FT, FR, CV, S1, S2, ACT, STB, SC, PG, T1, T2, R1, R2, OWN, PQ, taps, lsem,
    esend, erecv, wsend, wrecv, dsend, drecv, asend, arecv, rsend, rrecv, ssend, srecv, gsend, grecv, fsend, frecv,
):
    s = lax.axis_index("sp")
    x = lax.axis_index("tp")
    c = lax.rem(s, g.nc)
    y = lax.rem(lax.div(s, g.nc), g.ny)
    z = lax.div(s, g.nc * g.ny)
    sgn = 1 - 2 * c

    def rows_of(q, part=None):
        lo, n, _ = g.chunks[q]
        if part is None:
            return pl.ds(lo, n)
        return pl.ds(lo + part * (n // 2), n // 2)

    def sp_of(zz, yy, cc):
        return (zz * g.ny + yy) * g.nc + cc

    def at_x(j):
        return lax.rem(x + j + g.nx, g.nx)

    def remote(src, dst, send, recv, sp=None, tp=None):
        return pltpu.make_async_remote_copy(
            src_ref=src, dst_ref=dst, send_sem=send, recv_sem=recv,
            device_id=(s if sp is None else sp, x if tp is None else tp),
            device_id_type=MESH,
        )

    sent = []

    def go(copy):
        copy.start()
        sent.append(copy)

    size = {"y": g.ny, "z": g.nz}
    here = {"y": y, "z": z}

    def moved(axis, by):
        n = size[axis]
        return lax.rem(here[axis] + by + 2 * n, n)

    def ring_sp(axis, by):
        p = moved(axis, by)
        return sp_of(z, p, c) if axis == "y" else sp_of(p, y, c)

    partner = sp_of(z, y, 1 - c)
    after = lax.rem(s + 1, g.nsp)
    before = lax.rem(s + g.nsp - 1, g.nsp)

    loads = [(wv.at[i], WV.at[z, y, c, i]) for i in range(2)]
    loads += [(wg.at[i], WG.at[z, y, c, i]) for i in range(2)]
    loads += [(tok, X0.at[x])]
    loads += [(wo.at[i], WO.at[z, y, c, i]) for i in range(2)]
    loads += [(hbm_taps, taps)]
    loads = [pltpu.make_async_copy(a, b, lsem.at[i]) for i, (a, b) in enumerate(loads)]
    for load in loads:
        load.start()

    barrier = pltpu.get_barrier_semaphore()
    greet = [(None, at_x(j)) for j in range(1, g.nx)]
    greet += [(after, None), (before, None)]
    if g.nc > 1:
        greet.append((partner, None))
    for axis in ("y", "z"):
        greet += [(ring_sp(axis, k), None) for k in range(1, size[axis])]
    for sp, tp in greet:
        pl.semaphore_signal(
            barrier, inc=1,
            device_id=(s if sp is None else sp, x if tp is None else tp),
            device_id_type=MESH,
        )
    PG[x] = jnp.broadcast_to(pgain[0:1, :], (8, g.ch))
    STB[...] = jnp.zeros_like(STB)
    S1[...] = jnp.zeros_like(S1)
    S2[...] = jnp.zeros_like(S2)
    pl.semaphore_wait(barrier, len(greet))
    for load in loads[:-1]:
        load.wait()

    order = (("y", "z"), ("z", "y"))
    lanes = g.ch // 2
    pieces = {0: (0, 1), 1: (2,), 2: (3,), 3: (4,)}

    def source(item, stream):
        if item % 2 == 0:
            return (WV, WG)[stream], pl.ds(0, g.ch)
        return WO, pl.ds(stream * lanes, lanes)

    def own_slot(item, stream, pos):
        buf, cols = source(item, stream)
        zz, yy = (z, pos) if stream == 0 else (pos, y)
        return buf.at[zz, yy, c, item // 2, :, cols]

    def block(item, stream, pos, core, piece=None):
        buf, cols = source(item, stream)
        across_dim = slice(None)
        if piece is not None and len(pieces[item]) == 2:
            n = size[order[stream][0]] // 2
            near = lax.div(here[order[stream][0]], n)
            across_dim = pl.ds((near if piece == pieces[item][0] else 1 - near) * n, n)
        if stream == 0:
            return buf.at[pos, across_dim, core, item // 2, :, cols]
        return buf.at[across_dim, pos, core, item // 2, :, cols]

    def hops(axis):
        n = size[axis]
        return (n // 2, n - 1 - n // 2)

    def scatter_copy(item, stream, k):
        axis = order[stream][0]
        if k == 0:
            buf, cols = source(item, stream)
            some = pl.ds(0, size[axis] - 1)
            zz, yy = (z, some) if stream == 0 else (some, y)
            ref = buf.at[zz, yy, c, item // 2, :, cols]
        else:
            ref = own_slot(item, stream, here[axis])
        return remote(ref, ref, esend.at[item, stream], erecv.at[item, stream], sp=ring_sp(axis, max(k, 1)))

    def farthest_first(n):
        return sorted(range(1, n), key=lambda k: -min(k, n - k))

    def scatter(item):
        for k in farthest_first(max(g.ny, g.nz)):
            for stream in range(2):
                if k < size[order[stream][0]]:
                    scatter_copy(item, stream, k).start()
        for stream in range(2):
            if size[order[stream][0]] > 1:
                sent.append(scatter_copy(item, stream, 0))

    def scattered(item):
        for stream in range(2):
            if size[order[stream][0]] > 1:
                scatter_copy(item, stream, 0).wait_recv()

    def ring_copy(item, piece, stream, way, step, back):
        axis = order[stream][1]
        toward = sgn if way == 0 else -sgn
        ref = block(item, stream, moved(axis, -toward * (step + back)), c, piece)
        return remote(
            ref, ref,
            wsend.at[piece, stream],
            wrecv.at[piece, stream, way, step],
            sp=ring_sp(axis, toward),
        )

    def ring_sent(item, piece, stream):
        buf, cols = source(item, stream)
        first, second = (size[axis] for axis in order[stream])
        one, some = pl.ds(0, first // len(pieces[item])), pl.ds(0, second - 1)
        zz, yy = (some, one) if stream == 0 else (one, some)
        ref = buf.at[zz, yy, c, item // 2, :, cols]
        return remote(ref, ref, wsend.at[piece, stream], wrecv.at[piece, stream, 0, 0], sp=partner)

    def across(item, stream, pos=None):
        if pos is None:
            buf, cols = source(item, stream)
            ref = buf.at[:, :, c, item // 2, :, cols]
        else:
            ref = block(item, stream, pos, c)
        return remote(ref, ref, dsend.at[item, stream], drecv.at[item, stream], sp=partner)

    def begin(item):
        for piece in pieces[item]:
            for stream in range(2):
                axis = order[stream][1]
                for way in range(2):
                    if hops(axis)[way] > 0:
                        ring_copy(item, piece, stream, way, 0, 0).start()
                if size[axis] > 1:
                    sent.append(ring_sent(item, piece, stream))
        if g.nc > 1 and item < 2:
            for stream in range(2):
                across(item, stream, here[order[stream][1]]).start()

    def advance(item, step):
        for piece in pieces[item]:
            for stream in range(2):
                axis = order[stream][1]
                for way in range(2):
                    if step < hops(axis)[way]:
                        ring_copy(item, piece, stream, way, step, 1).wait_recv()
                        if step + 1 < hops(axis)[way]:
                            ring_copy(item, piece, stream, way, step + 1, 0).start()
                        if g.nc > 1 and item < 2 and piece == pieces[item][-1]:
                            toward = sgn if way == 0 else -sgn
                            across(item, stream, moved(axis, -toward * (step + 1))).start()
        if step == steps - 1 and g.nc > 1:
            for stream in range(2):
                if item >= 2:
                    across(item, stream).start()
                sent.append(across(item, stream))

    def finish(item):
        if g.nc > 1:
            for stream in range(2):
                buf, cols = source(item, stream)
                ref = buf.at[:, :, 1 - c, item // 2, :, cols]
                remote(ref, ref, dsend.at[item, stream], drecv.at[item, stream], sp=partner).wait_recv()

    steps = max(g.ny, g.nz) // 2

    def spread_copy(layer, q, buf, way, piece, back):
        toward = 1 - 2 * way
        origin = at_x(-toward * (back + (piece == 2)))
        ref = buf.at[origin, rows_of(q, 1 - way if piece == 1 else way)]
        return remote(
            ref, ref, asend.at[layer, q, way, piece], arecv.at[layer, q, way, piece], tp=at_x(toward)
        )

    def spread_begin(layer, q, buf):
        for piece in range(2):
            for way in range(2):
                go(spread_copy(layer, q, buf, way, piece, 0))

    def spread_relay(layer, q, buf):
        for way in range(2):
            spread_copy(layer, q, buf, way, 0, 1).wait_recv()
            go(spread_copy(layer, q, buf, way, 2, 0))

    def spread_end(layer, q, buf):
        for piece in (1, 2):
            for way in range(2):
                spread_copy(layer, q, buf, way, piece, 1).wait_recv()

    def tell(which):
        for j in range(1, g.nx):
            ref = STB.at[which, x]
            go(remote(ref, ref, ssend.at[which, j - 1], srecv.at[which, j - 1], tp=at_x(j)))

    def told(which):
        for j in range(1, g.nx):
            ref = STB.at[which, at_x(-j)]
            remote(ref, ref, ssend.at[which, j - 1], srecv.at[which, j - 1], tp=at_x(j)).wait_recv()

    def put_sums(which, row, buf, q):
        w = g.chunks[q][2]
        STB[which, x, row : row + 1, 0:w] = jnp.sum(jnp.transpose(buf[q, 0:w, :]), axis=0, keepdims=True)

    def as_columns(q, k, row):
        w = g.chunks[q][2]
        SC[q, k, 0:w, :] = jnp.transpose(jnp.broadcast_to(row, (128, w)))

    scatter(0)
    for q in range(2):
        spread_begin(0, q, X0)
    scatter(1)
    for j in range(1, g.nx):
        go(remote(PG.at[x], PG.at[x], gsend.at[j - 1], grecv.at[j - 1], tp=at_x(j)))
    scattered(0)
    begin(0)
    scattered(1)
    begin(1)
    scatter(2)
    scatter(3)
    for q in range(2):
        spread_relay(0, q, X0)
    advance(0, 0)
    advance(1, 0)
    for q in range(2):
        spread_end(0, q, X0)

    def loop(fn, lo, hi):
        def at(i, carry):
            fn(i)
            return carry

        lax.fori_loop(lo, hi, at, 0)

    def over(q, fn):
        lo, n, _ = g.chunks[q]
        loop(fn, lo // g.rb, (lo + n) // g.rb)

    def norm_rows(layer, i):
        rows = pl.ds(i * g.rb, g.rb)
        if layer == 1:
            square = jnp.zeros((g.rb, 1), F32)
            for j in range(g.nx):
                v = PJ[j, rows, :].astype(F32)
                square += jnp.sum(v * v, -1, keepdims=True)
            scale = lax.rsqrt(square / g.d + EPSILON)
        total = jnp.zeros((g.rb, 1), F32)
        for j in range(g.nx):
            v = X0[j, rows, :].astype(F32)
            if layer == 1:
                v = v + PJ[j, rows, :].astype(F32) * scale * PG[j, 0:1, :]
                X1[j, rows, :] = v.astype(BF16)
                v = v.astype(BF16).astype(F32)
            total += jnp.sum(v * v, -1, keepdims=True)
        inv = lax.rsqrt(total / g.d + EPSILON)
        for j in range(g.nx):
            v = (X0, X1)[layer][j, rows, :].astype(F32)
            cols = pl.ds(j * g.ch, g.ch)
            NB[rows, cols] = (v * inv * pre_gain[layer : layer + 1, cols]).astype(BF16)

    zs = g.nz // g.nx

    def project_in(layer, rows):
        for acc, w in ((AV, WV), (AG, WG)):
            mat = w[:, :, :, layer].reshape(g.d, g.ch)
            acc[rows, :] = jnp.dot(NB[rows, :], mat, preferred_element_type=F32)

    def gate(i):
        rows = pl.ds(i * g.rb, g.rb)
        for k in range(g.strips):
            cols = pl.ds(k * 128, 128)
            act = (AV[rows, cols] * jax.nn.sigmoid(AG[rows, cols])).astype(BF16)
            GF[k, pl.ds(HALO + i * g.rb, g.rb), :] = act.astype(F32)

    def fringe_copy(layer):
        return remote(FT.at[layer], FR.at[layer], fsend.at[layer], frecv.at[layer], sp=after)

    def fringe_send(layer):
        for k in range(g.strips):
            FT[layer, :, k * 128 : (k + 1) * 128] = GF[k, g.rows : g.rows + HALO, :].astype(BF16)
        go(fringe_copy(layer))

    def fringe_take(layer):
        fringe_copy(layer).wait_recv()
        keep = jnp.where(s > 0, 1.0, 0.0).astype(F32)
        for k in range(g.strips):
            GF[k, 0:HALO, :] = FR[layer, :, k * 128 : (k + 1) * 128].astype(F32) * keep

    def convolve(layer, q, i):
        whole = [jnp.zeros((g.rb, 128), F32) for _ in range(2)]
        for k in range(g.strips):
            cols = pl.ds(k * 128, 128)
            acc = jnp.zeros((g.rb, 128), F32)
            for tap in range(g.taps):
                rows = pl.ds(i * g.rb + (HALO - g.taps + 1 + tap), g.rb)
                acc = acc + taps[tap, layer : layer + 1, cols] * GF[k, rows, :]
            CV[k, pl.ds(i * g.rb, g.rb), :] = acc
            whole = [whole[0] + acc, whole[1] + acc * acc]
        local_rows = pl.ds(i * g.rb - g.chunks[q][0], g.rb)
        S1[q, local_rows, :] = whole[0]
        S2[q, local_rows, :] = whole[1]

    def activate(layer, q, i):
        rows = pl.ds(i * g.rb, g.rb)
        local_rows = pl.ds(i * g.rb - g.chunks[q][0], g.rb)
        center = SC[q, 0, local_rows, :]
        inv = SC[q, 1, local_rows, :]
        for k in range(g.strips):
            cols = pl.ds(k * 128, 128)
            v = (CV[k, rows, :] - center) * inv * ngain[layer : layer + 1, cols] + nshift[
                layer : layer + 1, cols
            ]
            ACT[rows, cols] = (v * jax.nn.sigmoid(v)).astype(BF16)

    def stats_send(layer, q):
        put_sums(2 * layer + q, 0, S1, q)
        put_sums(2 * layer + q, 1, S2, q)
        tell(2 * layer + q)

    def stats_take(layer, q):
        which, w = 2 * layer + q, g.chunks[q][2]
        told(which)
        sums = STB[which, 0, :, 0:w]
        for j in range(1, g.nx):
            sums = sums + STB[which, j, :, 0:w]
        center = sums[0:1, :] / g.d
        spread = jnp.maximum(sums[1:2, :] / g.d - center * center, 0.0)
        as_columns(q, 0, center)
        as_columns(q, 1, lax.rsqrt(spread + LN_EPSILON))

    def part_for(layer, q, dest):
        mat = WO[pl.ds(dest * zs, zs), :, :, layer].reshape(g.ch, g.ch)
        return lax.dot_general(
            ACT[rows_of(q), :], mat, (((1,), (1,)), ((), ())), preferred_element_type=F32
        )

    def far_hop(layer, q, way):
        part = rows_of(q, way)
        return remote(
            T1.at[layer, part], R1.at[layer, way, part],
            rsend.at[layer, q, way], rrecv.at[layer, q, way], tp=at_x(1 - 2 * way),
        )

    def near_hop(layer, q, way, added):
        part = rows_of(q, way if added else 1 - way)
        index = 2 + 2 * way + added
        return remote(
            T2.at[layer, way, part], R2.at[layer, way, part],
            rsend.at[layer, q, index], rrecv.at[layer, q, index], tp=at_x(1 - 2 * way),
        )

    def shares(layer, q):
        T1[layer, rows_of(q)] = part_for(layer, q, at_x(2)).astype(BF16)
        for way in range(2):
            go(far_hop(layer, q, way))
        for way in range(2):
            OWN[way, rows_of(q)] = part_for(layer, q, at_x(1 - 2 * way))
            part = rows_of(q, 1 - way)
            T2[layer, way, part] = OWN[way, part].astype(BF16)
            go(near_hop(layer, q, way, 0))

    def relay_shares(layer, q):
        for way in range(2):
            far_hop(layer, q, way).wait_recv()
            part = rows_of(q, way)
            T2[layer, way, part] = (OWN[way, part] + R1[layer, way, part].astype(F32)).astype(BF16)
            go(near_hop(layer, q, way, 1))

    def own_share(layer, q):
        OWN[2, rows_of(q)] = part_for(layer, q, x)

    def shares_end(layer, q):
        for added in range(2):
            for way in range(2):
                near_hop(layer, q, way, added).wait_recv()

        def combine(i):
            rows = pl.ds(i * g.rb, g.rb)
            v = (OWN[2, rows] + R2[layer, 0, rows].astype(F32) + R2[layer, 1, rows].astype(F32)).astype(BF16)
            if layer == 0:
                PJ[x, rows, :] = v
            else:
                PQ[rows, :] = v
                v = v.astype(F32)
                v = v * v
                S1[q, pl.ds(i * g.rb - g.chunks[q][0], g.rb), :] = sum(
                    v[:, k * 128 : (k + 1) * 128] for k in range(g.strips)
                )

        over(q, combine)

    A, B = 0, 1
    for layer in range(2):
        if layer == 0:
            loop(lambda i: norm_rows(0, i), 0, g.blocks)
            for step in range(1, steps):
                advance(0, step)
                advance(1, step)
            scattered(2)
            begin(2)
            scattered(3)
            begin(3)
            finish(0)
            project_in(0, pl.ds(0, g.rows))
            finish(1)
            over(A, gate)
            fringe_send(0)
            over(B, gate)
        else:
            spread_end(1, A, PJ)
            over(A, lambda i: norm_rows(1, i))
            finish(2)
            project_in(1, rows_of(A))
            over(A, gate)
            fringe_send(1)
            spread_end(1, B, PJ)
            over(B, lambda i: norm_rows(1, i))
            project_in(1, rows_of(B))
            over(B, gate)
            finish(3)
        if layer == 0:
            loads[-1].wait()
        over(A, lambda i: convolve(layer, A, i))
        stats_send(layer, A)
        loop(lambda i: convolve(layer, B, i), 1, g.split // g.rb)
        fringe_take(layer)
        loop(lambda i: convolve(layer, B, i), 0, 1)
        stats_send(layer, B)
        if layer == 0:
            advance(2, 0)
            advance(3, 0)
        stats_take(layer, A)
        over(A, lambda i: activate(layer, A, i))
        shares(layer, A)
        stats_take(layer, B)
        over(B, lambda i: activate(layer, B, i))
        shares(layer, B)
        relay_shares(layer, A)
        if layer == 0:
            advance(2, 1)
            advance(3, 1)
        own_share(layer, A)
        relay_shares(layer, B)
        own_share(layer, B)
        for q in (A, B):
            shares_end(layer, q)
            if layer == 0:
                spread_begin(1, q, PJ)
                advance(2, 2 + q)
                advance(3, 2 + q)
            else:
                put_sums(4 + q, 0, S1, q)
                tell(4 + q)
        if layer == 0:
            for j in range(1, g.nx):
                ref = PG.at[at_x(-j)]
                remote(ref, ref, gsend.at[j - 1], grecv.at[j - 1], tp=at_x(j)).wait_recv()
            for q in (A, B):
                spread_relay(1, q, PJ)

    for q in (A, B):
        told(4 + q)
        square = sum(STB[4 + q, j, 0:1, 0 : g.chunks[q][2]] for j in range(g.nx))
        as_columns(q, 0, lax.rsqrt(square / g.d + EPSILON))

        def last(i):
            rows = pl.ds(i * g.rb, g.rb)
            scale = SC[q, 0, pl.ds(i * g.rb - g.chunks[q][0], g.rb), :]
            for k in range(g.strips):
                cols = pl.ds(k * 128, 128)
                v = PQ[rows, cols].astype(F32) * scale * pgain[1:2, cols]
                out[rows, cols] = (X1[x, rows, cols].astype(F32) + v).astype(BF16)

        over(q, last)
    for copy in sent:
        copy.wait_send()


def local(g, tokens, pre_gain, w_value, w_gate, taps, norm_gain, norm_shift, w_out, post_gain):
    w_out = jnp.swapaxes(w_out, 1, 2)
    taps = jnp.swapaxes(taps, 0, 1)
    vm = pl.BlockSpec(memory_space=pltpu.VMEM)
    anywhere = pl.BlockSpec(memory_space=pl.ANY)
    slots = (g.nz, g.ny, g.nc, 2, g.kr, g.ch)
    rows, ch = g.rows, g.ch
    most = max(g.ny, g.nz)
    dma = pltpu.SemaphoreType.DMA
    scratch = [
        pltpu.VMEM(slots, BF16),
        pltpu.VMEM(slots, BF16),
        pltpu.VMEM(slots, BF16),
        pltpu.VMEM((g.nx, rows, ch), BF16),
        pltpu.VMEM((g.nx, rows, ch), BF16),
        pltpu.VMEM((g.nx, rows, ch), BF16),
        pltpu.VMEM((rows, g.d), BF16),
        pltpu.VMEM((rows, ch), F32),
        pltpu.VMEM((rows, ch), F32),
        pltpu.VMEM((g.strips, HALO + rows, 128), F32),
        pltpu.VMEM((2, HALO, ch), BF16),
        pltpu.VMEM((2, HALO, ch), BF16),
        pltpu.VMEM((g.strips, rows, 128), F32),
        pltpu.VMEM((2, g.wide, 128), F32),
        pltpu.VMEM((2, g.wide, 128), F32),
        pltpu.VMEM((rows, ch), BF16),
        pltpu.VMEM((6, g.nx, 8, g.wide), F32),
        pltpu.VMEM((2, 2, g.wide, 128), F32),
        pltpu.VMEM((g.nx, 8, ch), F32),
        pltpu.VMEM((2, rows, ch), BF16),
        pltpu.VMEM((2, 2, rows, ch), BF16),
        pltpu.VMEM((2, 2, rows, ch), BF16),
        pltpu.VMEM((2, 2, rows, ch), BF16),
        pltpu.VMEM((3, rows, ch), F32),
        pltpu.VMEM((rows, ch), BF16),
        pltpu.VMEM((g.taps, 2, ch), F32),
        dma((8,)),
        dma((4, 2)),
        dma((4, 2)),
        dma((5, 2)),
        dma((5, 2, 2, most // 2)),
        dma((4, 2)),
        dma((4, 2)),
        dma((2, 2, 2, 3)),
        dma((2, 2, 2, 3)),
        dma((2, 2, 6)),
        dma((2, 2, 6)),
        dma((6, 3)),
        dma((6, 3)),
        dma((3,)),
        dma((3,)),
        dma((2,)),
        dma((2,)),
    ]
    return pl.pallas_call(
        functools.partial(body, g),
        out_shape=jax.ShapeDtypeStruct((rows, ch), BF16),
        in_specs=[anywhere, vm, anywhere, anywhere, anywhere, vm, vm, anywhere, vm],
        out_specs=vm,
        scratch_shapes=scratch,
        compiler_params=pltpu.CompilerParams(
            collective_id=0, has_side_effects=True, vmem_limit_bytes=60 * 1024 * 1024
        ),
    )(tokens, pre_gain, w_value, w_gate, taps, norm_gain, norm_shift, w_out, post_gain)


def build(mesh, sizes, rows, ch, width):
    g = Geometry(*sizes, mesh.shape["tp"], rows, ch, width)
    placed = (
        P("sp", "tp"),
        P(),
        P(None, "sp", "tp"),
        P(None, "sp", "tp"),
        P(None, None, "tp"),
        P(None, "tp"),
        P(None, "tp"),
        P(None, "tp", "sp"),
        P(None, "tp"),
    )
    return jax.shard_map(
        functools.partial(local, g), mesh=mesh, in_specs=placed, out_specs=P("sp", "tp"), check_vma=False
    )


def solution(mesh):
    return build(mesh, (8, 8, 2), 320, 512, 31)
```

```python
import functools

import jax
import jax.numpy as jnp
from jax import lax
from jax.experimental import pallas as pl
from jax.experimental.pallas import tpu as pltpu
from jax.sharding import PartitionSpec as P

EPSILON = 1e-06
LN_EPSILON = 1e-05
HALO = 32
F32 = jnp.float32
BF16 = jnp.bfloat16
MESH = pl.DeviceIdType.MESH


class Geometry:
    def __init__(self, nz, ny, nc, nx, rows, ch, taps):
        self.nz, self.ny, self.nc, self.nx = nz, ny, nc, nx
        self.rows, self.ch, self.taps = rows, ch, taps
        self.d = ch * nx
        self.nsp = nz * ny * nc
        self.kr = self.d // self.nsp
        self.strips = ch // 128
        self.rb = 64
        self.blocks = rows // self.rb
        first = self.blocks // 2
        self.split = (self.blocks - first) * self.rb
        self.chunks = tuple((lo, n, -(-n // 128) * 128) for lo, n in ((self.split, rows - self.split), (0, self.split)))
        self.wide = max(w for _, _, w in self.chunks)


def body(
    g,
    tok, pre_gain, wv, wg, hbm_taps, ngain, nshift, wo, pgain,
    out,
    WV, WG, WO, X0, PJ, X1, NB, AV, AG, GF, FT, FR, CV, S1, S2, ACT, STB, SC, PG, T1, T2, R1, R2, OWN, PQ, taps, lsem,
    esend, erecv, wsend, wrecv, dsend, drecv, asend, arecv, rsend, rrecv, ssend, srecv, gsend, grecv, fsend, frecv,
):
    s = lax.axis_index("sp")
    x = lax.axis_index("tp")
    c = lax.rem(s, g.nc)
    y = lax.rem(lax.div(s, g.nc), g.ny)
    z = lax.div(s, g.nc * g.ny)
    sgn = 1 - 2 * c

    def rows_of(q, part=None):
        lo, n, _ = g.chunks[q]
        if part is None:
            return pl.ds(lo, n)
        return pl.ds(lo + part * (n // 2), n // 2)

    def sp_of(zz, yy, cc):
        return (zz * g.ny + yy) * g.nc + cc

    def at_x(j):
        return lax.rem(x + j + g.nx, g.nx)

    def remote(src, dst, send, recv, sp=None, tp=None):
        return pltpu.make_async_remote_copy(
            src_ref=src, dst_ref=dst, send_sem=send, recv_sem=recv,
            device_id=(s if sp is None else sp, x if tp is None else tp),
            device_id_type=MESH,
        )

    sent = []

    def go(copy):
        copy.start()
        sent.append(copy)

    size = {"y": g.ny, "z": g.nz}
    here = {"y": y, "z": z}

    def moved(axis, by):
        n = size[axis]
        return lax.rem(here[axis] + by + 2 * n, n)

    def ring_sp(axis, by):
        p = moved(axis, by)
        return sp_of(z, p, c) if axis == "y" else sp_of(p, y, c)

    partner = sp_of(z, y, 1 - c)
    after = lax.rem(s + 1, g.nsp)
    before = lax.rem(s + g.nsp - 1, g.nsp)

    loads = [(wv.at[i], WV.at[z, y, c, i]) for i in range(2)]
    loads += [(wg.at[i], WG.at[z, y, c, i]) for i in range(2)]
    loads += [(tok, X0.at[x])]
    loads += [(wo.at[i], WO.at[z, y, c, i]) for i in range(2)]
    loads += [(hbm_taps, taps)]
    loads = [pltpu.make_async_copy(a, b, lsem.at[i]) for i, (a, b) in enumerate(loads)]
    for load in loads:
        load.start()

    barrier = pltpu.get_barrier_semaphore()
    greet = [(None, at_x(j)) for j in range(1, g.nx)]
    greet += [(after, None), (before, None)]
    if g.nc > 1:
        greet.append((partner, None))
    for axis in ("y", "z"):
        greet += [(ring_sp(axis, k), None) for k in range(1, size[axis])]
    for sp, tp in greet:
        pl.semaphore_signal(
            barrier, inc=1,
            device_id=(s if sp is None else sp, x if tp is None else tp),
            device_id_type=MESH,
        )
    PG[x] = jnp.broadcast_to(pgain[0:1, :], (8, g.ch))
    STB[...] = jnp.zeros_like(STB)
    S1[...] = jnp.zeros_like(S1)
    S2[...] = jnp.zeros_like(S2)
    pl.semaphore_wait(barrier, len(greet))
    for load in loads[:-1]:
        load.wait()

    order = (("y", "z"), ("z", "y"))
    lanes = g.ch // 2
    pieces = {0: (0, 1), 1: (2,), 2: (3,), 3: (4,)}

    def source(item, stream):
        if item % 2 == 0:
            return (WV, WG)[stream], pl.ds(0, g.ch)
        return WO, pl.ds(stream * lanes, lanes)

    def own_slot(item, stream, pos):
        buf, cols = source(item, stream)
        zz, yy = (z, pos) if stream == 0 else (pos, y)
        return buf.at[zz, yy, c, item // 2, :, cols]

    def block(item, stream, pos, core, piece=None):
        buf, cols = source(item, stream)
        across_dim = slice(None)
        if piece is not None and len(pieces[item]) == 2:
            n = size[order[stream][0]] // 2
            near = lax.div(here[order[stream][0]], n)
            across_dim = pl.ds((near if piece == pieces[item][0] else 1 - near) * n, n)
        if stream == 0:
            return buf.at[pos, across_dim, core, item // 2, :, cols]
        return buf.at[across_dim, pos, core, item // 2, :, cols]

    def hops(axis):
        n = size[axis]
        return (n // 2, n - 1 - n // 2)

    def scatter_copy(item, stream, k):
        axis = order[stream][0]
        if k == 0:
            buf, cols = source(item, stream)
            some = pl.ds(0, size[axis] - 1)
            zz, yy = (z, some) if stream == 0 else (some, y)
            ref = buf.at[zz, yy, c, item // 2, :, cols]
        else:
            ref = own_slot(item, stream, here[axis])
        return remote(ref, ref, esend.at[item, stream], erecv.at[item, stream], sp=ring_sp(axis, max(k, 1)))

    def farthest_first(n):
        return sorted(range(1, n), key=lambda k: -min(k, n - k))

    def scatter(item):
        for k in farthest_first(max(g.ny, g.nz)):
            for stream in range(2):
                if k < size[order[stream][0]]:
                    scatter_copy(item, stream, k).start()
        for stream in range(2):
            if size[order[stream][0]] > 1:
                sent.append(scatter_copy(item, stream, 0))

    def scattered(item):
        for stream in range(2):
            if size[order[stream][0]] > 1:
                scatter_copy(item, stream, 0).wait_recv()

    def ring_copy(item, piece, stream, way, step, back):
        axis = order[stream][1]
        toward = sgn if way == 0 else -sgn
        ref = block(item, stream, moved(axis, -toward * (step + back)), c, piece)
        return remote(
            ref, ref,
            wsend.at[piece, stream],
            wrecv.at[piece, stream, way, step],
            sp=ring_sp(axis, toward),
        )

    def ring_sent(item, piece, stream):
        buf, cols = source(item, stream)
        first, second = (size[axis] for axis in order[stream])
        one, some = pl.ds(0, first // len(pieces[item])), pl.ds(0, second - 1)
        zz, yy = (some, one) if stream == 0 else (one, some)
        ref = buf.at[zz, yy, c, item // 2, :, cols]
        return remote(ref, ref, wsend.at[piece, stream], wrecv.at[piece, stream, 0, 0], sp=partner)

    def across(item, stream, pos=None):
        if pos is None:
            buf, cols = source(item, stream)
            ref = buf.at[:, :, c, item // 2, :, cols]
        else:
            ref = block(item, stream, pos, c)
        return remote(ref, ref, dsend.at[item, stream], drecv.at[item, stream], sp=partner)

    def begin(item):
        for piece in pieces[item]:
            for stream in range(2):
                axis = order[stream][1]
                for way in range(2):
                    if hops(axis)[way] > 0:
                        ring_copy(item, piece, stream, way, 0, 0).start()
                if size[axis] > 1:
                    sent.append(ring_sent(item, piece, stream))
        if g.nc > 1 and item < 2:
            for stream in range(2):
                across(item, stream, here[order[stream][1]]).start()

    def advance(item, step):
        for piece in pieces[item]:
            for stream in range(2):
                axis = order[stream][1]
                for way in range(2):
                    if step < hops(axis)[way]:
                        ring_copy(item, piece, stream, way, step, 1).wait_recv()
                        if step + 1 < hops(axis)[way]:
                            ring_copy(item, piece, stream, way, step + 1, 0).start()
                        if g.nc > 1 and item < 2 and piece == pieces[item][-1]:
                            toward = sgn if way == 0 else -sgn
                            across(item, stream, moved(axis, -toward * (step + 1))).start()
        if step == steps - 1 and g.nc > 1:
            for stream in range(2):
                if item >= 2:
                    across(item, stream).start()
                sent.append(across(item, stream))

    def finish(item):
        if g.nc > 1:
            for stream in range(2):
                buf, cols = source(item, stream)
                ref = buf.at[:, :, 1 - c, item // 2, :, cols]
                remote(ref, ref, dsend.at[item, stream], drecv.at[item, stream], sp=partner).wait_recv()

    steps = max(g.ny, g.nz) // 2

    def spread_copy(layer, q, buf, way, piece, back):
        toward = 1 - 2 * way
        origin = at_x(-toward * (back + (piece == 2)))
        ref = buf.at[origin, rows_of(q, 1 - way if piece == 1 else way)]
        return remote(
            ref, ref, asend.at[layer, q, way, piece], arecv.at[layer, q, way, piece], tp=at_x(toward)
        )

    def spread_begin(layer, q, buf):
        for piece in range(2):
            for way in range(2):
                go(spread_copy(layer, q, buf, way, piece, 0))

    def spread_relay(layer, q, buf):
        for way in range(2):
            spread_copy(layer, q, buf, way, 0, 1).wait_recv()
            go(spread_copy(layer, q, buf, way, 2, 0))

    def spread_end(layer, q, buf):
        for piece in (1, 2):
            for way in range(2):
                spread_copy(layer, q, buf, way, piece, 1).wait_recv()

    def tell(which):
        for j in range(1, g.nx):
            ref = STB.at[which, x]
            go(remote(ref, ref, ssend.at[which, j - 1], srecv.at[which, j - 1], tp=at_x(j)))

    def told(which):
        for j in range(1, g.nx):
            ref = STB.at[which, at_x(-j)]
            remote(ref, ref, ssend.at[which, j - 1], srecv.at[which, j - 1], tp=at_x(j)).wait_recv()

    def put_sums(which, row, buf, q):
        w = g.chunks[q][2]
        STB[which, x, row : row + 1, 0:w] = jnp.sum(jnp.transpose(buf[q, 0:w, :]), axis=0, keepdims=True)

    def as_columns(q, k, row):
        w = g.chunks[q][2]
        SC[q, k, 0:w, :] = jnp.transpose(jnp.broadcast_to(row, (128, w)))

    scatter(0)
    for q in range(2):
        spread_begin(0, q, X0)
    scatter(1)
    for j in range(1, g.nx):
        go(remote(PG.at[x], PG.at[x], gsend.at[j - 1], grecv.at[j - 1], tp=at_x(j)))
    scattered(0)
    begin(0)
    scattered(1)
    begin(1)
    scatter(2)
    scatter(3)
    for q in range(2):
        spread_relay(0, q, X0)
    advance(0, 0)
    advance(1, 0)
    for q in range(2):
        spread_end(0, q, X0)

    def loop(fn, lo, hi):
        def at(i, carry):
            fn(i)
            return carry

        lax.fori_loop(lo, hi, at, 0)

    def over(q, fn):
        lo, n, _ = g.chunks[q]
        loop(fn, lo // g.rb, (lo + n) // g.rb)

    def lane_groups(v):
        return sum(v[:, k * 128 : (k + 1) * 128] * v[:, k * 128 : (k + 1) * 128] for k in range(g.strips))

    def norm_rows(layer, i):
        rows = pl.ds(i * g.rb, g.rb)
        if layer == 1:
            square = jnp.zeros((g.rb, 128), F32)
            for j in range(g.nx):
                square += lane_groups(PJ[j, rows, :].astype(F32))
            scale = lax.rsqrt(jnp.sum(square, -1, keepdims=True) / g.d + EPSILON)
        total = jnp.zeros((g.rb, 128), F32)
        for j in range(g.nx):
            v = X0[j, rows, :].astype(F32)
            if layer == 1:
                v = v + PJ[j, rows, :].astype(F32) * scale * PG[j, 0:1, :]
                X1[j, rows, :] = v.astype(BF16)
                v = v.astype(BF16).astype(F32)
            total += lane_groups(v)
        inv = lax.rsqrt(jnp.sum(total, -1, keepdims=True) / g.d + EPSILON)
        for j in range(g.nx):
            v = (X0, X1)[layer][j, rows, :].astype(F32)
            cols = pl.ds(j * g.ch, g.ch)
            NB[rows, cols] = (v * inv * pre_gain[layer : layer + 1, cols]).astype(BF16)

    zs = g.nz // g.nx

    def project_in(layer, rows):
        for acc, w in ((AV, WV), (AG, WG)):
            mat = w[:, :, :, layer].reshape(g.d, g.ch)
            acc[rows, :] = jnp.dot(NB[rows, :], mat, preferred_element_type=F32)

    def gate(i):
        rows = pl.ds(i * g.rb, g.rb)
        for k in range(g.strips):
            cols = pl.ds(k * 128, 128)
            act = (AV[rows, cols] * jax.nn.sigmoid(AG[rows, cols])).astype(BF16)
            GF[k, pl.ds(HALO + i * g.rb, g.rb), :] = act.astype(F32)

    def fringe_copy(layer):
        return remote(FT.at[layer], FR.at[layer], fsend.at[layer], frecv.at[layer], sp=after)

    def fringe_send(layer):
        for k in range(g.strips):
            FT[layer, :, k * 128 : (k + 1) * 128] = GF[k, g.rows : g.rows + HALO, :].astype(BF16)
        go(fringe_copy(layer))

    def fringe_take(layer):
        fringe_copy(layer).wait_recv()
        keep = jnp.where(s > 0, 1.0, 0.0).astype(F32)
        for k in range(g.strips):
            GF[k, 0:HALO, :] = FR[layer, :, k * 128 : (k + 1) * 128].astype(F32) * keep

    def convolve(layer, q, i):
        whole = [jnp.zeros((g.rb, 128), F32) for _ in range(2)]
        for k in range(g.strips):
            cols = pl.ds(k * 128, 128)
            acc = jnp.zeros((g.rb, 128), F32)
            for tap in range(g.taps):
                rows = pl.ds(i * g.rb + (HALO - g.taps + 1 + tap), g.rb)
                acc = acc + taps[tap, layer : layer + 1, cols] * GF[k, rows, :]
            CV[k, pl.ds(i * g.rb, g.rb), :] = acc
            whole = [whole[0] + acc, whole[1] + acc * acc]
        local_rows = pl.ds(i * g.rb - g.chunks[q][0], g.rb)
        S1[q, local_rows, :] = whole[0]
        S2[q, local_rows, :] = whole[1]

    def activate(layer, q, i):
        rows = pl.ds(i * g.rb, g.rb)
        local_rows = pl.ds(i * g.rb - g.chunks[q][0], g.rb)
        center = SC[q, 0, local_rows, :]
        inv = SC[q, 1, local_rows, :]
        for k in range(g.strips):
            cols = pl.ds(k * 128, 128)
            v = (CV[k, rows, :] - center) * inv * ngain[layer : layer + 1, cols] + nshift[
                layer : layer + 1, cols
            ]
            ACT[rows, cols] = (v * jax.nn.sigmoid(v)).astype(BF16)

    def stats_send(layer, q):
        put_sums(2 * layer + q, 0, S1, q)
        put_sums(2 * layer + q, 1, S2, q)
        tell(2 * layer + q)

    def stats_take(layer, q):
        which, w = 2 * layer + q, g.chunks[q][2]
        told(which)
        sums = STB[which, 0, :, 0:w]
        for j in range(1, g.nx):
            sums = sums + STB[which, j, :, 0:w]
        center = sums[0:1, :] / g.d
        spread = jnp.maximum(sums[1:2, :] / g.d - center * center, 0.0)
        as_columns(q, 0, center)
        as_columns(q, 1, lax.rsqrt(spread + LN_EPSILON))

    def part_for(layer, q, dest):
        mat = WO[pl.ds(dest * zs, zs), :, :, layer].reshape(g.ch, g.ch)
        return lax.dot_general(
            ACT[rows_of(q), :], mat, (((1,), (1,)), ((), ())), preferred_element_type=F32
        )

    def far_hop(layer, q, way):
        part = rows_of(q, way)
        return remote(
            T1.at[layer, part], R1.at[layer, way, part],
            rsend.at[layer, q, way], rrecv.at[layer, q, way], tp=at_x(1 - 2 * way),
        )

    def near_hop(layer, q, way, added):
        part = rows_of(q, way if added else 1 - way)
        index = 2 + 2 * way + added
        return remote(
            T2.at[layer, way, part], R2.at[layer, way, part],
            rsend.at[layer, q, index], rrecv.at[layer, q, index], tp=at_x(1 - 2 * way),
        )

    def shares(layer, q):
        T1[layer, rows_of(q)] = part_for(layer, q, at_x(2)).astype(BF16)
        for way in range(2):
            go(far_hop(layer, q, way))
        for way in range(2):
            OWN[way, rows_of(q)] = part_for(layer, q, at_x(1 - 2 * way))
            part = rows_of(q, 1 - way)
            T2[layer, way, part] = OWN[way, part].astype(BF16)
            go(near_hop(layer, q, way, 0))

    def relay_shares(layer, q):
        for way in range(2):
            far_hop(layer, q, way).wait_recv()
            part = rows_of(q, way)
            T2[layer, way, part] = (OWN[way, part] + R1[layer, way, part].astype(F32)).astype(BF16)
            go(near_hop(layer, q, way, 1))

    def own_share(layer, q):
        OWN[2, rows_of(q)] = part_for(layer, q, x)

    def shares_end(layer, q):
        for added in range(2):
            for way in range(2):
                near_hop(layer, q, way, added).wait_recv()

        def combine(i):
            rows = pl.ds(i * g.rb, g.rb)
            v = (OWN[2, rows] + R2[layer, 0, rows].astype(F32) + R2[layer, 1, rows].astype(F32)).astype(BF16)
            if layer == 0:
                PJ[x, rows, :] = v
            else:
                PQ[rows, :] = v
                v = v.astype(F32)
                v = v * v
                S1[q, pl.ds(i * g.rb - g.chunks[q][0], g.rb), :] = sum(
                    v[:, k * 128 : (k + 1) * 128] for k in range(g.strips)
                )

        over(q, combine)

    A, B = 0, 1
    early = g.split // g.rb + 1
    for layer in range(2):
        if layer == 0:
            loop(lambda i: norm_rows(0, i), 0, g.blocks)
            for step in range(1, steps):
                advance(0, step)
                advance(1, step)
            scattered(2)
            begin(2)
            scattered(3)
            begin(3)
            finish(0)
            project_in(0, pl.ds(0, g.rows))
            finish(1)
            over(A, gate)
            fringe_send(0)
            over(B, gate)
        else:
            spread_end(1, A, PJ)
            over(A, lambda i: norm_rows(1, i))
            finish(2)
            project_in(1, rows_of(A))
            over(A, gate)
            fringe_send(1)
            loop(lambda i: convolve(1, A, i), early, g.blocks)
            spread_end(1, B, PJ)
            over(B, lambda i: norm_rows(1, i))
            project_in(1, rows_of(B))
            over(B, gate)
            finish(3)
        if layer == 0:
            loads[-1].wait()
        loop(lambda i: convolve(layer, A, i), early - 1, g.blocks if layer == 0 else early)
        stats_send(layer, A)
        loop(lambda i: convolve(layer, B, i), 1, g.split // g.rb)
        fringe_take(layer)
        loop(lambda i: convolve(layer, B, i), 0, 1)
        stats_send(layer, B)
        if layer == 0:
            advance(2, 0)
            advance(3, 0)
        stats_take(layer, A)
        over(A, lambda i: activate(layer, A, i))
        shares(layer, A)
        stats_take(layer, B)
        over(B, lambda i: activate(layer, B, i))
        shares(layer, B)
        relay_shares(layer, A)
        if layer == 0:
            advance(2, 1)
            advance(3, 1)
        own_share(layer, A)
        relay_shares(layer, B)
        own_share(layer, B)
        for q in (A, B):
            shares_end(layer, q)
            if layer == 0:
                spread_begin(1, q, PJ)
                advance(2, 2 + q)
                advance(3, 2 + q)
            else:
                put_sums(4 + q, 0, S1, q)
                tell(4 + q)
        if layer == 0:
            for j in range(1, g.nx):
                ref = PG.at[at_x(-j)]
                remote(ref, ref, gsend.at[j - 1], grecv.at[j - 1], tp=at_x(j)).wait_recv()
            for q in (A, B):
                spread_relay(1, q, PJ)

    for q in (A, B):
        told(4 + q)
        square = sum(STB[4 + q, j, 0:1, 0 : g.chunks[q][2]] for j in range(g.nx))
        as_columns(q, 0, lax.rsqrt(square / g.d + EPSILON))

        def last(i):
            rows = pl.ds(i * g.rb, g.rb)
            scale = SC[q, 0, pl.ds(i * g.rb - g.chunks[q][0], g.rb), :]
            for k in range(g.strips):
                cols = pl.ds(k * 128, 128)
                v = PQ[rows, cols].astype(F32) * scale * pgain[1:2, cols]
                out[rows, cols] = (X1[x, rows, cols].astype(F32) + v).astype(BF16)

        over(q, last)
    for copy in sent:
        copy.wait_send()


def local(g, tokens, pre_gain, w_value, w_gate, taps, norm_gain, norm_shift, w_out, post_gain):
    w_out = jnp.swapaxes(w_out, 1, 2)
    taps = jnp.swapaxes(taps, 0, 1)
    vm = pl.BlockSpec(memory_space=pltpu.VMEM)
    anywhere = pl.BlockSpec(memory_space=pl.ANY)
    slots = (g.nz, g.ny, g.nc, 2, g.kr, g.ch)
    rows, ch = g.rows, g.ch
    most = max(g.ny, g.nz)
    dma = pltpu.SemaphoreType.DMA
    scratch = [
        pltpu.VMEM(slots, BF16),
        pltpu.VMEM(slots, BF16),
        pltpu.VMEM(slots, BF16),
        pltpu.VMEM((g.nx, rows, ch), BF16),
        pltpu.VMEM((g.nx, rows, ch), BF16),
        pltpu.VMEM((g.nx, rows, ch), BF16),
        pltpu.VMEM((rows, g.d), BF16),
        pltpu.VMEM((rows, ch), F32),
        pltpu.VMEM((rows, ch), F32),
        pltpu.VMEM((g.strips, HALO + rows, 128), F32),
        pltpu.VMEM((2, HALO, ch), BF16),
        pltpu.VMEM((2, HALO, ch), BF16),
        pltpu.VMEM((g.strips, rows, 128), F32),
        pltpu.VMEM((2, g.wide, 128), F32),
        pltpu.VMEM((2, g.wide, 128), F32),
        pltpu.VMEM((rows, ch), BF16),
        pltpu.VMEM((6, g.nx, 8, g.wide), F32),
        pltpu.VMEM((2, 2, g.wide, 128), F32),
        pltpu.VMEM((g.nx, 8, ch), F32),
        pltpu.VMEM((2, rows, ch), BF16),
        pltpu.VMEM((2, 2, rows, ch), BF16),
        pltpu.VMEM((2, 2, rows, ch), BF16),
        pltpu.VMEM((2, 2, rows, ch), BF16),
        pltpu.VMEM((3, rows, ch), F32),
        pltpu.VMEM((rows, ch), BF16),
        pltpu.VMEM((g.taps, 2, ch), F32),
        dma((8,)),
        dma((4, 2)),
        dma((4, 2)),
        dma((5, 2)),
        dma((5, 2, 2, most // 2)),
        dma((4, 2)),
        dma((4, 2)),
        dma((2, 2, 2, 3)),
        dma((2, 2, 2, 3)),
        dma((2, 2, 6)),
        dma((2, 2, 6)),
        dma((6, 3)),
        dma((6, 3)),
        dma((3,)),
        dma((3,)),
        dma((2,)),
        dma((2,)),
    ]
    return pl.pallas_call(
        functools.partial(body, g),
        out_shape=jax.ShapeDtypeStruct((rows, ch), BF16),
        in_specs=[anywhere, vm, anywhere, anywhere, anywhere, vm, vm, anywhere, vm],
        out_specs=vm,
        scratch_shapes=scratch,
        compiler_params=pltpu.CompilerParams(
            collective_id=0, has_side_effects=True, vmem_limit_bytes=60 * 1024 * 1024
        ),
    )(tokens, pre_gain, w_value, w_gate, taps, norm_gain, norm_shift, w_out, post_gain)


def build(mesh, sizes, rows, ch, width):
    g = Geometry(*sizes, mesh.shape["tp"], rows, ch, width)
    placed = (
        P("sp", "tp"),
        P(),
        P(None, "sp", "tp"),
        P(None, "sp", "tp"),
        P(None, None, "tp"),
        P(None, "tp"),
        P(None, "tp"),
        P(None, "tp", "sp"),
        P(None, "tp"),
    )
    return jax.shard_map(
        functools.partial(local, g), mesh=mesh, in_specs=placed, out_specs=P("sp", "tp"), check_vma=False
    )


def solution(mesh):
    return build(mesh, (8, 8, 2), 320, 512, 31)
```

```python
import functools

import jax
import jax.numpy as jnp
from jax import lax
from jax.experimental import pallas as pl
from jax.experimental.pallas import tpu as pltpu
from jax.sharding import PartitionSpec as P

EPSILON = 1e-06
LN_EPSILON = 1e-05
HALO = 32
F32 = jnp.float32
BF16 = jnp.bfloat16
MESH = pl.DeviceIdType.MESH


class Geometry:
    def __init__(self, nz, ny, nc, nx, rows, ch, taps):
        self.nz, self.ny, self.nc, self.nx = nz, ny, nc, nx
        self.rows, self.ch, self.taps = rows, ch, taps
        self.d = ch * nx
        self.nsp = nz * ny * nc
        self.kr = self.d // self.nsp
        self.strips = ch // 128
        self.rb = 64
        self.blocks = rows // self.rb
        first = self.blocks // 2
        self.split = (self.blocks - first) * self.rb
        self.chunks = tuple((lo, n, -(-n // 128) * 128) for lo, n in ((self.split, rows - self.split), (0, self.split)))
        self.wide = max(w for _, _, w in self.chunks)


def body(
    g,
    tok, pre_gain, wv, wg, hbm_taps, ngain, nshift, wo, pgain,
    out,
    WV, WG, WO, X0, PJ, X1, NB, AV, AG, GF, FT, FR, CV, S1, S2, ACT, STB, SC, PG, T1, T2, R1, R2, OWN, PQ, taps, lsem,
    esend, erecv, wsend, wrecv, dsend, drecv, asend, arecv, rsend, rrecv, ssend, srecv, gsend, grecv, fsend, frecv,
):
    s = lax.axis_index("sp")
    x = lax.axis_index("tp")
    c = lax.rem(s, g.nc)
    y = lax.rem(lax.div(s, g.nc), g.ny)
    z = lax.div(s, g.nc * g.ny)
    sgn = 1 - 2 * c

    def rows_of(q, part=None):
        lo, n, _ = g.chunks[q]
        if part is None:
            return pl.ds(lo, n)
        return pl.ds(lo + part * (n // 2), n // 2)

    def sp_of(zz, yy, cc):
        return (zz * g.ny + yy) * g.nc + cc

    def at_x(j):
        return lax.rem(x + j + g.nx, g.nx)

    def remote(src, dst, send, recv, sp=None, tp=None):
        return pltpu.make_async_remote_copy(
            src_ref=src, dst_ref=dst, send_sem=send, recv_sem=recv,
            device_id=(s if sp is None else sp, x if tp is None else tp),
            device_id_type=MESH,
        )

    sent = []

    def go(copy):
        copy.start()
        sent.append(copy)

    size = {"y": g.ny, "z": g.nz}
    here = {"y": y, "z": z}

    def moved(axis, by):
        n = size[axis]
        return lax.rem(here[axis] + by + 2 * n, n)

    def ring_sp(axis, by):
        p = moved(axis, by)
        return sp_of(z, p, c) if axis == "y" else sp_of(p, y, c)

    partner = sp_of(z, y, 1 - c)
    after = lax.rem(s + 1, g.nsp)
    before = lax.rem(s + g.nsp - 1, g.nsp)

    loads = [(wv.at[i], WV.at[z, y, c, i]) for i in range(2)]
    loads += [(wg.at[i], WG.at[z, y, c, i]) for i in range(2)]
    loads += [(tok, X0.at[x])]
    loads += [(wo.at[i], WO.at[z, y, c, i]) for i in range(2)]
    loads += [(hbm_taps, taps)]
    loads = [pltpu.make_async_copy(a, b, lsem.at[i]) for i, (a, b) in enumerate(loads)]
    for load in loads:
        load.start()

    barrier = pltpu.get_barrier_semaphore()
    greet = [(None, at_x(j)) for j in range(1, g.nx)]
    greet += [(after, None), (before, None)]
    if g.nc > 1:
        greet.append((partner, None))
    for axis in ("y", "z"):
        greet += [(ring_sp(axis, k), None) for k in range(1, size[axis])]
    for sp, tp in greet:
        pl.semaphore_signal(
            barrier, inc=1,
            device_id=(s if sp is None else sp, x if tp is None else tp),
            device_id_type=MESH,
        )
    PG[x] = jnp.broadcast_to(pgain[0:1, :], (8, g.ch))
    STB[...] = jnp.zeros_like(STB)
    S1[...] = jnp.zeros_like(S1)
    S2[...] = jnp.zeros_like(S2)
    pl.semaphore_wait(barrier, len(greet))
    for load in loads[:-1]:
        load.wait()

    order = (("y", "z"), ("z", "y"))
    lanes = g.ch // 2
    pieces = {0: (0, 1), 1: (2,), 2: (3,), 3: (4,)}

    def source(item, stream):
        if item % 2 == 0:
            return (WV, WG)[stream], pl.ds(0, g.ch)
        return WO, pl.ds(stream * lanes, lanes)

    def own_slot(item, stream, pos):
        buf, cols = source(item, stream)
        zz, yy = (z, pos) if stream == 0 else (pos, y)
        return buf.at[zz, yy, c, item // 2, :, cols]

    def block(item, stream, pos, core, piece=None):
        buf, cols = source(item, stream)
        across_dim = slice(None)
        if piece is not None and len(pieces[item]) == 2:
            n = size[order[stream][0]] // 2
            near = lax.div(here[order[stream][0]], n)
            across_dim = pl.ds((near if piece == pieces[item][0] else 1 - near) * n, n)
        if stream == 0:
            return buf.at[pos, across_dim, core, item // 2, :, cols]
        return buf.at[across_dim, pos, core, item // 2, :, cols]

    def hops(axis):
        n = size[axis]
        return (n // 2, n - 1 - n // 2)

    def scatter_copy(item, stream, k):
        axis = order[stream][0]
        if k == 0:
            buf, cols = source(item, stream)
            some = pl.ds(0, size[axis] - 1)
            zz, yy = (z, some) if stream == 0 else (some, y)
            ref = buf.at[zz, yy, c, item // 2, :, cols]
        else:
            ref = own_slot(item, stream, here[axis])
        return remote(ref, ref, esend.at[item, stream], erecv.at[item, stream], sp=ring_sp(axis, max(k, 1)))

    def farthest_first(n):
        return sorted(range(1, n), key=lambda k: -min(k, n - k))

    def scatter(item):
        for k in farthest_first(max(g.ny, g.nz)):
            for stream in range(2):
                if k < size[order[stream][0]]:
                    scatter_copy(item, stream, k).start()
        for stream in range(2):
            if size[order[stream][0]] > 1:
                sent.append(scatter_copy(item, stream, 0))

    def scattered(item):
        for stream in range(2):
            if size[order[stream][0]] > 1:
                scatter_copy(item, stream, 0).wait_recv()

    def ring_copy(item, piece, stream, way, step, back):
        axis = order[stream][1]
        toward = sgn if way == 0 else -sgn
        ref = block(item, stream, moved(axis, -toward * (step + back)), c, piece)
        return remote(
            ref, ref,
            wsend.at[piece, stream],
            wrecv.at[piece, stream, way, step],
            sp=ring_sp(axis, toward),
        )

    def ring_sent(item, piece, stream):
        buf, cols = source(item, stream)
        first, second = (size[axis] for axis in order[stream])
        one, some = pl.ds(0, first // len(pieces[item])), pl.ds(0, second - 1)
        zz, yy = (some, one) if stream == 0 else (one, some)
        ref = buf.at[zz, yy, c, item // 2, :, cols]
        return remote(ref, ref, wsend.at[piece, stream], wrecv.at[piece, stream, 0, 0], sp=partner)

    def across(item, stream, pos=None):
        if pos is None:
            buf, cols = source(item, stream)
            ref = buf.at[:, :, c, item // 2, :, cols]
        else:
            ref = block(item, stream, pos, c)
        return remote(ref, ref, dsend.at[item, stream], drecv.at[item, stream], sp=partner)

    def begin(item):
        for piece in pieces[item]:
            for stream in range(2):
                axis = order[stream][1]
                for way in range(2):
                    if hops(axis)[way] > 0:
                        ring_copy(item, piece, stream, way, 0, 0).start()
                if size[axis] > 1:
                    sent.append(ring_sent(item, piece, stream))
        if g.nc > 1 and item < 2:
            for stream in range(2):
                across(item, stream, here[order[stream][1]]).start()

    def advance(item, step):
        for piece in pieces[item]:
            for stream in range(2):
                axis = order[stream][1]
                for way in range(2):
                    if step < hops(axis)[way]:
                        ring_copy(item, piece, stream, way, step, 1).wait_recv()
                        if step + 1 < hops(axis)[way]:
                            ring_copy(item, piece, stream, way, step + 1, 0).start()
                        if g.nc > 1 and item < 2 and piece == pieces[item][-1]:
                            toward = sgn if way == 0 else -sgn
                            across(item, stream, moved(axis, -toward * (step + 1))).start()
        if step == steps - 1 and g.nc > 1:
            for stream in range(2):
                if item >= 2:
                    across(item, stream).start()
                sent.append(across(item, stream))

    def finish(item):
        if g.nc > 1:
            for stream in range(2):
                buf, cols = source(item, stream)
                ref = buf.at[:, :, 1 - c, item // 2, :, cols]
                remote(ref, ref, dsend.at[item, stream], drecv.at[item, stream], sp=partner).wait_recv()

    steps = max(g.ny, g.nz) // 2

    def spread_copy(layer, q, buf, way, piece, back):
        toward = 1 - 2 * way
        origin = at_x(-toward * (back + (piece == 2)))
        ref = buf.at[origin, rows_of(q, 1 - way if piece == 1 else way)]
        return remote(
            ref, ref, asend.at[layer, q, way, piece], arecv.at[layer, q, way, piece], tp=at_x(toward)
        )

    def spread_begin(layer, q, buf):
        for piece in range(2):
            for way in range(2):
                go(spread_copy(layer, q, buf, way, piece, 0))

    def spread_relay(layer, q, buf):
        for way in range(2):
            spread_copy(layer, q, buf, way, 0, 1).wait_recv()
            go(spread_copy(layer, q, buf, way, 2, 0))

    def spread_end(layer, q, buf):
        for piece in (1, 2):
            for way in range(2):
                spread_copy(layer, q, buf, way, piece, 1).wait_recv()

    def tell(which):
        for j in range(1, g.nx):
            ref = STB.at[which, x]
            go(remote(ref, ref, ssend.at[which, j - 1], srecv.at[which, j - 1], tp=at_x(j)))

    def told(which):
        for j in range(1, g.nx):
            ref = STB.at[which, at_x(-j)]
            remote(ref, ref, ssend.at[which, j - 1], srecv.at[which, j - 1], tp=at_x(j)).wait_recv()

    def put_sums(which, row, buf, q):
        w = g.chunks[q][2]
        STB[which, x, row : row + 1, 0:w] = jnp.sum(jnp.transpose(buf[q, 0:w, :]), axis=0, keepdims=True)

    def as_columns(q, k, row):
        w = g.chunks[q][2]
        SC[q, k, 0:w, :] = jnp.transpose(jnp.broadcast_to(row, (128, w)))

    scatter(0)
    for q in range(2):
        spread_begin(0, q, X0)
    scatter(1)
    for j in range(1, g.nx):
        go(remote(PG.at[x], PG.at[x], gsend.at[j - 1], grecv.at[j - 1], tp=at_x(j)))
    scattered(0)
    begin(0)
    scattered(1)
    begin(1)
    scatter(2)
    scatter(3)
    for q in range(2):
        spread_relay(0, q, X0)
    advance(0, 0)
    advance(1, 0)
    for q in range(2):
        spread_end(0, q, X0)

    def loop(fn, lo, hi):
        def at(i, carry):
            fn(i)
            return carry

        lax.fori_loop(lo, hi, at, 0)

    def over(q, fn):
        lo, n, _ = g.chunks[q]
        loop(fn, lo // g.rb, (lo + n) // g.rb)

    def lane_groups(v):
        return sum(v[:, k * 128 : (k + 1) * 128] * v[:, k * 128 : (k + 1) * 128] for k in range(g.strips))

    def norm_rows(layer, i):
        rows = pl.ds(i * g.rb, g.rb)
        if layer == 1:
            square = jnp.zeros((g.rb, 128), F32)
            for j in range(g.nx):
                square += lane_groups(PJ[j, rows, :].astype(F32))
            scale = lax.rsqrt(jnp.sum(square, -1, keepdims=True) / g.d + EPSILON)
        total = jnp.zeros((g.rb, 128), F32)
        for j in range(g.nx):
            v = X0[j, rows, :].astype(F32)
            if layer == 1:
                v = v + PJ[j, rows, :].astype(F32) * scale * PG[j, 0:1, :]
                X1[j, rows, :] = v.astype(BF16)
                v = v.astype(BF16).astype(F32)
            total += lane_groups(v)
        inv = lax.rsqrt(jnp.sum(total, -1, keepdims=True) / g.d + EPSILON)
        for j in range(g.nx):
            v = (X0, X1)[layer][j, rows, :].astype(F32)
            cols = pl.ds(j * g.ch, g.ch)
            NB[rows, cols] = (v * inv * pre_gain[layer : layer + 1, cols]).astype(BF16)

    zs = g.nz // g.nx

    def project_in(layer, rows):
        for acc, w in ((AV, WV), (AG, WG)):
            mat = w[:, :, :, layer].reshape(g.d, g.ch)
            acc[rows, :] = jnp.dot(NB[rows, :], mat, preferred_element_type=F32)

    def gate(i):
        rows = pl.ds(i * g.rb, g.rb)
        for k in range(g.strips):
            cols = pl.ds(k * 128, 128)
            act = (AV[rows, cols] * jax.nn.sigmoid(AG[rows, cols])).astype(BF16)
            GF[k, pl.ds(HALO + i * g.rb, g.rb), :] = act.astype(F32)

    def fringe_copy(layer):
        return remote(FT.at[layer], FR.at[layer], fsend.at[layer], frecv.at[layer], sp=after)

    def fringe_send(layer):
        for k in range(g.strips):
            FT[layer, :, k * 128 : (k + 1) * 128] = GF[k, g.rows : g.rows + HALO, :].astype(BF16)
        go(fringe_copy(layer))

    def fringe_take(layer):
        fringe_copy(layer).wait_recv()
        keep = jnp.where(s > 0, 1.0, 0.0).astype(F32)
        for k in range(g.strips):
            GF[k, 0:HALO, :] = FR[layer, :, k * 128 : (k + 1) * 128].astype(F32) * keep

    def convolve(layer, q, i):
        whole = [jnp.zeros((g.rb, 128), F32) for _ in range(2)]
        for k in range(g.strips):
            cols = pl.ds(k * 128, 128)
            acc = jnp.zeros((g.rb, 128), F32)
            for tap in range(g.taps):
                rows = pl.ds(i * g.rb + (HALO - g.taps + 1 + tap), g.rb)
                acc = acc + taps[tap, layer : layer + 1, cols] * GF[k, rows, :]
            CV[k, pl.ds(i * g.rb, g.rb), :] = acc
            whole = [whole[0] + acc, whole[1] + acc * acc]
        local_rows = pl.ds(i * g.rb - g.chunks[q][0], g.rb)
        S1[q, local_rows, :] = whole[0]
        S2[q, local_rows, :] = whole[1]

    def activate(layer, q, i):
        rows = pl.ds(i * g.rb, g.rb)
        local_rows = pl.ds(i * g.rb - g.chunks[q][0], g.rb)
        center = SC[q, 0, local_rows, :]
        inv = SC[q, 1, local_rows, :]
        for k in range(g.strips):
            cols = pl.ds(k * 128, 128)
            v = (CV[k, rows, :] - center) * inv * ngain[layer : layer + 1, cols] + nshift[
                layer : layer + 1, cols
            ]
            ACT[rows, cols] = (v * jax.nn.sigmoid(v)).astype(BF16)

    def stats_send(layer, q):
        put_sums(2 * layer + q, 0, S1, q)
        put_sums(2 * layer + q, 1, S2, q)
        tell(2 * layer + q)

    def stats_take(layer, q):
        which, w = 2 * layer + q, g.chunks[q][2]
        told(which)
        sums = STB[which, 0, :, 0:w]
        for j in range(1, g.nx):
            sums = sums + STB[which, j, :, 0:w]
        center = sums[0:1, :] / g.d
        spread = jnp.maximum(sums[1:2, :] / g.d - center * center, 0.0)
        as_columns(q, 0, center)
        as_columns(q, 1, lax.rsqrt(spread + LN_EPSILON))

    def part_for(layer, q, dest):
        mat = WO[pl.ds(dest * zs, zs), :, :, layer].reshape(g.ch, g.ch)
        return lax.dot_general(
            ACT[rows_of(q), :], mat, (((1,), (1,)), ((), ())), preferred_element_type=F32
        )

    def far_hop(layer, q, way):
        part = rows_of(q, way)
        return remote(
            T1.at[layer, part], R1.at[layer, way, part],
            rsend.at[layer, q, way], rrecv.at[layer, q, way], tp=at_x(1 - 2 * way),
        )

    def near_hop(layer, q, way, added):
        part = rows_of(q, way if added else 1 - way)
        index = 2 + 2 * way + added
        return remote(
            T2.at[layer, way, part], R2.at[layer, way, part],
            rsend.at[layer, q, index], rrecv.at[layer, q, index], tp=at_x(1 - 2 * way),
        )

    def shares(layer, q):
        T1[layer, rows_of(q)] = part_for(layer, q, at_x(2)).astype(BF16)
        for way in range(2):
            go(far_hop(layer, q, way))
        for way in range(2):
            OWN[way, rows_of(q)] = part_for(layer, q, at_x(1 - 2 * way))
            part = rows_of(q, 1 - way)
            T2[layer, way, part] = OWN[way, part].astype(BF16)
            go(near_hop(layer, q, way, 0))

    def relay_shares(layer, q):
        for way in range(2):
            far_hop(layer, q, way).wait_recv()
            part = rows_of(q, way)
            T2[layer, way, part] = (OWN[way, part] + R1[layer, way, part].astype(F32)).astype(BF16)
            go(near_hop(layer, q, way, 1))

    def own_share(layer, q):
        OWN[2, rows_of(q)] = part_for(layer, q, x)

    def shares_end(layer, q):
        for added in range(2):
            for way in range(2):
                near_hop(layer, q, way, added).wait_recv()

        def combine(i):
            rows = pl.ds(i * g.rb, g.rb)
            v = (OWN[2, rows] + R2[layer, 0, rows].astype(F32) + R2[layer, 1, rows].astype(F32)).astype(BF16)
            if layer == 0:
                PJ[x, rows, :] = v
            else:
                PQ[rows, :] = v
                v = v.astype(F32)
                v = v * v
                S1[q, pl.ds(i * g.rb - g.chunks[q][0], g.rb), :] = sum(
                    v[:, k * 128 : (k + 1) * 128] for k in range(g.strips)
                )

        over(q, combine)

    A, B = 0, 1
    early = g.split // g.rb + 1
    for layer in range(2):
        if layer == 0:
            loop(lambda i: norm_rows(0, i), 0, g.blocks)
            for step in range(1, steps):
                advance(0, step)
                advance(1, step)
            scattered(2)
            begin(2)
            scattered(3)
            begin(3)
            finish(0)
            project_in(0, pl.ds(0, g.rows))
            finish(1)
            over(A, gate)
            fringe_send(0)
            over(B, gate)
        else:
            spread_end(1, A, PJ)
            over(A, lambda i: norm_rows(1, i))
            finish(2)
            project_in(1, rows_of(A))
            over(A, gate)
            fringe_send(1)
            loop(lambda i: convolve(1, A, i), early, g.blocks)
            spread_end(1, B, PJ)
            over(B, lambda i: norm_rows(1, i))
            project_in(1, rows_of(B))
            over(B, gate)
            finish(3)
        if layer == 0:
            loads[-1].wait()
        loop(lambda i: convolve(layer, A, i), early - 1, g.blocks if layer == 0 else early)
        stats_send(layer, A)
        loop(lambda i: convolve(layer, B, i), 1, g.split // g.rb)
        fringe_take(layer)
        loop(lambda i: convolve(layer, B, i), 0, 1)
        stats_send(layer, B)
        if layer == 0:
            advance(2, 0)
            advance(3, 0)
        stats_take(layer, A)
        over(A, lambda i: activate(layer, A, i))
        shares(layer, A)
        stats_take(layer, B)
        over(B, lambda i: activate(layer, B, i))
        shares(layer, B)
        relay_shares(layer, A)
        own_share(layer, A)
        relay_shares(layer, B)
        own_share(layer, B)
        if layer == 0:
            advance(2, 1)
            advance(3, 1)
        for q in (A, B):
            shares_end(layer, q)
            if layer == 0:
                spread_begin(1, q, PJ)
                advance(2, 2 + q)
                advance(3, 2 + q)
            else:
                put_sums(4 + q, 0, S1, q)
                tell(4 + q)
        if layer == 0:
            for j in range(1, g.nx):
                ref = PG.at[at_x(-j)]
                remote(ref, ref, gsend.at[j - 1], grecv.at[j - 1], tp=at_x(j)).wait_recv()
            for q in (A, B):
                spread_relay(1, q, PJ)

    for q in (A, B):
        told(4 + q)
        square = sum(STB[4 + q, j, 0:1, 0 : g.chunks[q][2]] for j in range(g.nx))
        as_columns(q, 0, lax.rsqrt(square / g.d + EPSILON))

        def last(i):
            rows = pl.ds(i * g.rb, g.rb)
            scale = SC[q, 0, pl.ds(i * g.rb - g.chunks[q][0], g.rb), :]
            for k in range(g.strips):
                cols = pl.ds(k * 128, 128)
                v = PQ[rows, cols].astype(F32) * scale * pgain[1:2, cols]
                out[rows, cols] = (X1[x, rows, cols].astype(F32) + v).astype(BF16)

        over(q, last)
    for copy in sent:
        copy.wait_send()


def local(g, tokens, pre_gain, w_value, w_gate, taps, norm_gain, norm_shift, w_out, post_gain):
    w_out = jnp.swapaxes(w_out, 1, 2)
    taps = jnp.swapaxes(taps, 0, 1)
    vm = pl.BlockSpec(memory_space=pltpu.VMEM)
    anywhere = pl.BlockSpec(memory_space=pl.ANY)
    slots = (g.nz, g.ny, g.nc, 2, g.kr, g.ch)
    rows, ch = g.rows, g.ch
    most = max(g.ny, g.nz)
    dma = pltpu.SemaphoreType.DMA
    scratch = [
        pltpu.VMEM(slots, BF16),
        pltpu.VMEM(slots, BF16),
        pltpu.VMEM(slots, BF16),
        pltpu.VMEM((g.nx, rows, ch), BF16),
        pltpu.VMEM((g.nx, rows, ch), BF16),
        pltpu.VMEM((g.nx, rows, ch), BF16),
        pltpu.VMEM((rows, g.d), BF16),
        pltpu.VMEM((rows, ch), F32),
        pltpu.VMEM((rows, ch), F32),
        pltpu.VMEM((g.strips, HALO + rows, 128), F32),
        pltpu.VMEM((2, HALO, ch), BF16),
        pltpu.VMEM((2, HALO, ch), BF16),
        pltpu.VMEM((g.strips, rows, 128), F32),
        pltpu.VMEM((2, g.wide, 128), F32),
        pltpu.VMEM((2, g.wide, 128), F32),
        pltpu.VMEM((rows, ch), BF16),
        pltpu.VMEM((6, g.nx, 8, g.wide), F32),
        pltpu.VMEM((2, 2, g.wide, 128), F32),
        pltpu.VMEM((g.nx, 8, ch), F32),
        pltpu.VMEM((2, rows, ch), BF16),
        pltpu.VMEM((2, 2, rows, ch), BF16),
        pltpu.VMEM((2, 2, rows, ch), BF16),
        pltpu.VMEM((2, 2, rows, ch), BF16),
        pltpu.VMEM((3, rows, ch), F32),
        pltpu.VMEM((rows, ch), BF16),
        pltpu.VMEM((g.taps, 2, ch), F32),
        dma((8,)),
        dma((4, 2)),
        dma((4, 2)),
        dma((5, 2)),
        dma((5, 2, 2, most // 2)),
        dma((4, 2)),
        dma((4, 2)),
        dma((2, 2, 2, 3)),
        dma((2, 2, 2, 3)),
        dma((2, 2, 6)),
        dma((2, 2, 6)),
        dma((6, 3)),
        dma((6, 3)),
        dma((3,)),
        dma((3,)),
        dma((2,)),
        dma((2,)),
    ]
    return pl.pallas_call(
        functools.partial(body, g),
        out_shape=jax.ShapeDtypeStruct((rows, ch), BF16),
        in_specs=[anywhere, vm, anywhere, anywhere, anywhere, vm, vm, anywhere, vm],
        out_specs=vm,
        scratch_shapes=scratch,
        compiler_params=pltpu.CompilerParams(
            collective_id=0, has_side_effects=True, vmem_limit_bytes=60 * 1024 * 1024
        ),
    )(tokens, pre_gain, w_value, w_gate, taps, norm_gain, norm_shift, w_out, post_gain)


def build(mesh, sizes, rows, ch, width):
    g = Geometry(*sizes, mesh.shape["tp"], rows, ch, width)
    placed = (
        P("sp", "tp"),
        P(),
        P(None, "sp", "tp"),
        P(None, "sp", "tp"),
        P(None, None, "tp"),
        P(None, "tp"),
        P(None, "tp"),
        P(None, "tp", "sp"),
        P(None, "tp"),
    )
    return jax.shard_map(
        functools.partial(local, g), mesh=mesh, in_specs=placed, out_specs=P("sp", "tp"), check_vma=False
    )


def solution(mesh):
    return build(mesh, (8, 8, 2), 320, 512, 31)
```
